32 devices in a mesh: sp: 16 (over z, y, x), tp: 2 (over core).
Axes of the slice: x: 2, y: 2, z: 4, core: 2. Of those that a mesh axis runs over, the one named last changes fastest.
Arguments:
- conv_in: bfloat16 [4096, 1024], P('sp', 'tp'), may hold values from -6 to 6
- gate_outer: bfloat16 [4096, 1024], P('sp', 'tp'), may hold values from -6 to 6
- gate_inner: bfloat16 [4096, 1024], P('sp', 'tp'), may hold values from -6 to 6
- tap_weights: float32 [3, 1024], P(None, 'tp'), may hold values from -3 to 3
- doc_ids: int32 [4096], P('sp'), may hold values from 0 to 7, never falling along the last dimension, each value on 1 to 1024 neighbouring positions
- w_proj: bfloat16 [1024, 2048], replicated, may hold values from -0.1875 to 0.1875
- stream: bfloat16 [4096, 2048], P(('sp', 'tp')), may hold values from -6 to 6
- norm_gain: float32 [2048], replicated, may hold values from 0.1 to 1.9
- routes: int32 [4096, 4], P(('sp', 'tp')), may hold values from 0 to 31, all different within a row; in each aligned block of 128 rows (0 to 127, 128 to 255, ...) at most 32 rows name the same one
- route_weights: float32 [4096, 4], P(('sp', 'tp')), may hold values from 0.1 to 1
- w_gate: bfloat16 [32, 2048, 768], P(('sp', 'tp')), may hold values from -0.5 to 0.5
- w_up: bfloat16 [32, 2048, 768], P(('sp', 'tp')), may hold values from -0.5 to 0.5
- w_down: bfloat16 [32, 768, 2048], P(('sp', 'tp')), may hold values from -0.0546875 to 0.0546875
Outputs:
- layer_out: bfloat16 [4096, 2048], P(('sp', 'tp'))
The draws below stay inside these ranges and needn't reach their ends.
Inputs may be any that keep to these rules, and one draw needn't show every extreme that they name: `doc_ids`: document numbers never fall along the sequence; a document covers at most 1024 positions. `routes`: a token names 4 different experts; among the rows of one device (aligned blocks of 128 tokens) no expert is named more than 32 times, a bound that some block reaches.
All inputs are finite; a program needn't handle non-finite values.
Results may differ from the reference program's by a relative error of at most 0.0071.
Values may be sent and summed in bfloat16 or wider, within the bound.
A program may use at most 128 MiB of HBM per device.

```python
import math
import jax
import jax.numpy as jnp
import numpy as np
from jax import lax

D = 2048
CW = 1024
FF = 768
TOPK = 4
TAPS = 3
TOK_DEV = 256
TOKENS = 4096
EXPERTS = 32
BLOCK = 128
CAP = 32
DOCS = 8
DOC_MOST = 1024
N_TP = 2


def block_scale(own_key, dims, split, low, top_value):
    def one(position, blocks):
        draws = jax.random.uniform(jax.random.fold_in(jax.random.fold_in(own_key, 6), position), (blocks,), jnp.float32, low / len(split), top_value / len(split))
        return jnp.repeat(jnp.exp(draws), dims[position] // blocks).reshape((-1,) + (1,) * (len(dims) - position - 1))

    factor_of = one(*split[0])
    for cut in split[1:]:
        factor_of = factor_of * one(*cut)
    return factor_of


def split_up(number_of, total, most, skew):
    portions = [(1 << 20) // math.isqrt(rank ** skew) + 1 for rank in range(2, number_of + 1)]
    rest, holding = total - most - (number_of - 1), [1] * (number_of - 1)
    while rest > 0:
        movable = [i for i in range(number_of - 1) if holding[i] < most]
        whole, remaining = sum([portions[i] for i in movable]), rest
        for i in movable:
            extra = min(most - holding[i], max(1, remaining * portions[i] // whole), rest)
            holding[i] = holding[i] + extra
            rest = rest - extra
    return np.array([most] + holding)


def ragged(own_key, count, total, bound, lean):
    if count == 2:
        one = jax.random.randint(own_key, (), max(1, total - bound), min(bound, total - 1) + 1)
        return jnp.stack([one, total - one])
    sizes = jnp.asarray(split_up(count, total, bound, lean), jnp.int32)
    twos = (count - 1) // 2
    giver, taker = sizes[1:1 + 2 * twos:2], sizes[2:2 + 2 * twos:2]
    margin = jnp.minimum(giver - 1, bound - taker)
    passed = jax.random.randint(jax.random.fold_in(own_key, 1), (twos,), 0, 1 << 20) % (margin + 1)
    sizes = sizes.at[1:1 + 2 * twos:2].set(giver - passed).at[2:2 + 2 * twos:2].set(taker + passed)
    return sizes[jax.random.permutation(jax.random.fold_in(own_key, 2), count)]


def shared_out(own_key, own, number, rows, amount, top, most, slope):
    ranking = jax.random.permutation(own_key, amount)
    heavy_load, common = portions_of(amount, rows * top, most, slope, True), portions_of(amount, rows * top, most, slope, False)
    places = jnp.arange(amount)

    def named(lengths, offset_by):
        used = int((lengths > 0).sum())
        fixed = max(1, used // 4)
        moved = fixed + (places - fixed + offset_by * (used - fixed)) % max(1, amount - fixed)
        return jnp.zeros((amount,), jnp.int32).at[ranking[jnp.where(places < fixed, places, moved)]].set(jnp.asarray(lengths, jnp.int32))

    lengths = jnp.where(number % 4 == 0, named(heavy_load, number // 4), named(common, number - number // 4 - 1))
    mixed = jax.random.permutation(jax.random.fold_in(own, 3), amount)
    donor, sink = mixed[0:amount // 2 * 2:2], mixed[1:amount // 2 * 2:2]
    room = jnp.minimum(lengths[donor] - 1, most - lengths[sink]) // 2
    room = jnp.where((donor == ranking[0]) | (sink == ranking[0]) | (lengths[sink] == 0), 0, jnp.maximum(room, 0))
    moved = jax.random.randint(jax.random.fold_in(own, 4), (amount // 2,), 0, 1 << 20) % (room + 1)
    lengths = lengths.at[donor].add(-moved).at[sink].add(moved)
    members = jnp.searchsorted(jnp.cumsum(lengths), jnp.arange(rows * top), side="right").astype(jnp.int32)
    table = members.reshape(top, rows).T
    table = table[jax.random.permutation(jax.random.fold_in(own, 1), rows)]
    offset_by = jax.random.randint(jax.random.fold_in(own, 2), (rows, 1), 0, top)
    return jnp.take_along_axis(table, (jnp.arange(top)[None, :] + offset_by) % top, axis=1)


def portions_of(amount, total, most, skew, full):
    portions = [(1 << 20) // math.isqrt(grade ** skew) + 1 for grade in range(1, amount + 1)]
    largest = most if full else min(most, max(-(-total // amount), total * portions[0] // sum(portions)))
    least = 1 if total - largest >= amount - 1 else 0
    holding, rest = [largest] + [least] * (amount - 1), total - largest - least * (amount - 1)
    while rest > 0:
        free = [i for i in range(1, amount) if holding[i] < largest] or [i for i in range(1, amount) if holding[i] < most]
        pool, remaining = sum([portions[i] for i in free]), rest
        for i in free:
            more = min(most - holding[i], max(1, remaining * portions[i] // pool), rest)
            holding[i] = holding[i] + more
            rest = rest - more
    return np.array(holding)


def noise(rng, shape, width, limit, pieces=(), held_as=jnp.bfloat16):
    entries = width * jax.random.normal(rng, shape, jnp.float32)
    if pieces:
        entries = entries * block_scale(rng, shape, pieces, -0.22, 0.18)
    return jnp.clip(entries, -limit, limit).astype(held_as)


def setup_inputs(seed: int = 0) -> dict:
    arg_keys = jax.random.split(jax.random.key(seed), 14)
    conv_in = noise(arg_keys[0], (TOKENS, CW), 1.0, 6.0, ((0, 16), (1, 2)))
    gate_outer = noise(arg_keys[1], (TOKENS, CW), 1.0, 6.0, ((0, 16), (1, 2)))
    gate_inner = noise(arg_keys[2], (TOKENS, CW), 1.0, 6.0, ((0, 16), (1, 2)))
    tap_weights = noise(arg_keys[3], (TAPS, CW), 0.6, 3.0, ((1, 2),), jnp.float32)
    doc_ids = jnp.searchsorted(jnp.cumsum(ragged(arg_keys[4], DOCS, TOKENS, DOC_MOST, 0)), jnp.arange(TOKENS), side="right").astype(jnp.int32)
    w_proj = noise(arg_keys[5], (CW, D), CW ** -0.5, 0.1875)
    stream = noise(arg_keys[6], (TOKENS, D), 1.0, 6.0, ((0, 32),))
    norm_gain = jnp.clip(1.0 + 0.18 * jax.random.normal(arg_keys[7], (D,), jnp.float32), 0.1, 1.9)
    routes_keys = jax.random.split(jax.random.fold_in(arg_keys[8], 1), TOKENS // BLOCK)
    routes_turns = jax.random.permutation(jax.random.fold_in(arg_keys[8], 3), TOKENS // BLOCK)
    routes = jax.vmap(lambda own, number: shared_out(jax.random.fold_in(arg_keys[8], 2), own, number, BLOCK, EXPERTS, TOPK, CAP, 1))(routes_keys, routes_turns).reshape((TOKENS, TOPK))
    route_weights = jnp.clip(jnp.exp(math.log(1.0) - 2.3025851 * jax.random.uniform(arg_keys[9], (TOKENS, TOPK), jnp.float32) ** block_scale(arg_keys[9], (TOKENS, TOPK), ((0, 32),), -0.2, 0.2)), 0.1, 1.0)
    w_gate = noise(arg_keys[10], (EXPERTS, D, FF), (D // 16) ** -0.5, 0.5, ((0, 32),))
    w_up = noise(arg_keys[11], (EXPERTS, D, FF), (D // 16) ** -0.5, 0.5, ((0, 32),))
    w_down = noise(arg_keys[12], (EXPERTS, FF, D), (16 * FF) ** -0.5, 0.0546875, ((0, 32),))
    return dict(conv_in=conv_in, gate_outer=gate_outer, gate_inner=gate_inner, tap_weights=tap_weights, doc_ids=doc_ids, w_proj=w_proj, stream=stream, norm_gain=norm_gain, routes=routes, route_weights=route_weights, w_gate=w_gate, w_up=w_up, w_down=w_down)


def expert_rows(rows, wg, wu, wd):
    gate = jnp.minimum(jnp.dot(rows, wg, preferred_element_type=jnp.float32), 7.0)
    upper = jnp.clip(jnp.dot(rows, wu, preferred_element_type=jnp.float32), -7.0, 7.0)
    act = ((upper + 1.0) * gate * jax.nn.sigmoid(1.702 * gate)).astype(jnp.bfloat16)
    return jnp.dot(act, wd, preferred_element_type=jnp.float32).astype(jnp.bfloat16)

def reference(conv_in, gate_outer, gate_inner, tap_weights, doc_ids, w_proj, stream, norm_gain, routes, route_weights, w_gate, w_up, w_down):
    product = gate_inner.astype(jnp.float32) * conv_in.astype(jnp.float32)
    same = (doc_ids[1:] == doc_ids[:-1]).astype(jnp.float32)
    zero_row = jnp.zeros((1, product.shape[1]), jnp.float32)
    before = jnp.concatenate([zero_row, product[:-1] * same[:, None]], axis=0)
    after = jnp.concatenate([product[1:] * same[:, None], zero_row], axis=0)
    conv = tap_weights[0] * before + tap_weights[1] * product + tap_weights[2] * after
    mixed = (gate_outer.astype(jnp.float32) * conv).astype(jnp.bfloat16)
    hidden = stream.astype(jnp.float32) + jnp.dot(mixed, w_proj, preferred_element_type=jnp.float32)
    scale = lax.rsqrt(lax.optimization_barrier(jnp.mean(hidden * hidden, axis=-1, keepdims=True)) + 1e-05)
    normed = (hidden * scale * norm_gain).astype(jnp.bfloat16)
    block = TOK_DEV // N_TP
    nblocks = TOKENS // block
    slots = nblocks * CAP
    chosen = routes.reshape(nblocks, block * TOPK)
    onehot = (chosen[:, :, None] == jnp.arange(EXPERTS, dtype=jnp.int32)[None, None, :]).astype(jnp.int32)
    ranks = lax.optimization_barrier(jnp.sum(jnp.cumsum(onehot, axis=1) * onehot, axis=-1)) - 1
    block_ids = jnp.arange(nblocks, dtype=jnp.int32)[:, None]
    places = (chosen * slots + block_ids * CAP + ranks).reshape(-1).astype(jnp.int32)
    owners = (block_ids * block + (jnp.arange(block * TOPK, dtype=jnp.int32) // TOPK)[None, :]).reshape(-1)
    table = jnp.full((EXPERTS * slots,), TOKENS, jnp.int32).at[places].set(owners).reshape(EXPERTS, slots)
    weights = jnp.zeros((EXPERTS * slots,), jnp.float32).at[places].set(route_weights.reshape(-1)).reshape(EXPERTS, slots)
    padded = jnp.concatenate([normed, jnp.zeros((1, normed.shape[1]), jnp.bfloat16)], axis=0)

    def one_expert(total, items):
        owner_ids, owner_weights, wg, wu, wd = items
        result = expert_rows(padded[owner_ids], wg, wu, wd)
        total = total.at[owner_ids].add(result.astype(jnp.float32) * owner_weights[:, None])
        return (total, None)
    start = jnp.zeros((TOKENS + 1, normed.shape[1]), jnp.float32)
    total, _ = lax.scan(one_expert, start, (table, weights, w_gate, w_up, w_down))
    return (hidden + total[:TOKENS]).astype(jnp.bfloat16)
```

```python
import functools
import math

import jax
import jax.numpy as jnp
from jax import lax
from jax.experimental import pallas as pl
from jax.experimental.pallas import tpu as pltpu
from jax.sharding import PartitionSpec as P

MESH = pl.DeviceIdType.MESH
HALO = 16
BF = jnp.bfloat16
F32 = jnp.float32


def dot(a, b):
    return jnp.dot(a, b, preferred_element_type=F32)


def tile_of(size, most):
    return next(t for t in range(most, 0, -128) if size % t == 0)


def nearest_first(nz):
    return [sorted(range(nz), key=lambda b: (abs(b - z), abs(2 * b - nz + 1) * (1 if nz > 2 else 0), b))
            for z in range(nz)]


def layer_kernel(
    n_seq, nz, n_plane, n_core, cap, col,
    ci_hbm, go_hbm, gi_hbm, taps_hbm, docs_hbm, wp_hbm, stream_hbm, gain_hbm,
    routes_hbm, rw_hbm, wg_hbm, wu_hbm, wd_hbm,
    out_ref,
    wg, wu, wd, wp, ci_f, gi_f, go_f, taps_f, docs, prod, mixed, stream, gain, hidden,
    rbuf, wbuf, select, spread, zbuf, outgoing, arrived, act, returned, partial, summed,
    l_sem, e_send, e_recv, h_send, h_recv, d_send, d_recv, rt_send, rt_recv,
    zu_send, zd_send, z_recv, a_send, a_recv, r_send, r_recv, p_send, p_recv,
):
    peers = n_plane * n_core
    rows = peers * cap
    block, width = hidden.shape
    ff = wg.shape[1]
    half = ci_hbm.shape[1]
    span = block + HALO
    nc = width // col
    me = lax.axis_index("sp")
    core = lax.axis_index("tp")
    z, p = me // n_plane, lax.rem(me, n_plane)
    rank = p * n_core + core
    other = 1 - core

    def at_z(b):
        return {"sp": b * n_plane + p, "tp": core}

    def plane_peer(j):
        q = lax.rem(rank + j, peers)
        return {"sp": z * n_plane + q // n_core, "tp": lax.rem(q, n_core)}

    nxt, prv = lax.rem(me + 1, n_seq), lax.rem(me + n_seq - 1, n_seq)
    order = nearest_first(nz)

    def ordered(k):
        total = jnp.int32(0)
        for i in range(nz):
            total = total + jnp.where(z == i, order[i][k], 0)
        return total

    def remote(src, dst, send, recv, to):
        return pltpu.make_async_remote_copy(
            src_ref=src, dst_ref=dst, send_sem=send, recv_sem=recv,
            device_id=to, device_id_type=MESH)

    mine = pl.multiple_of(core * (block - HALO), HALO)
    theirs = pl.multiple_of(other * (block - HALO), HALO)
    my_at = pl.multiple_of(other * HALO, HALO)
    their_at = pl.multiple_of(core * HALO, HALO)

    def local(i, src, dst):
        return pltpu.make_async_copy(src, dst, l_sem.at[i])

    front = [
        local(0, ci_hbm.at[pl.ds(mine, span)], ci_f.at[core, pl.ds(my_at, span)]),
        local(1, gi_hbm.at[pl.ds(mine, span)], gi_f.at[core, pl.ds(my_at, span)]),
        local(2, go_hbm.at[pl.ds(pl.multiple_of(core * block, HALO), block)], go_f.at[core]),
        local(3, taps_hbm, taps_f.at[core]),
        local(4, docs_hbm, docs.at[0]),
        local(5, stream_hbm, stream),
        local(6, gain_hbm, gain),
    ]
    tables = [local(7, routes_hbm, rbuf.at[z]), local(8, rw_hbm, wbuf.at[z])]
    project = local(9, wp_hbm, wp)
    weights = [local(10, wg_hbm, wg), local(11, wu_hbm, wu), local(12, wd_hbm, wd)]
    for load in front + tables + [project]:
        load.start()

    barrier = pltpu.get_barrier_semaphore()

    def greet(to):
        pl.semaphore_signal(barrier, inc=1, device_id=to, device_id_type=MESH)

    for k in range(1, nz):
        greet(at_z(lax.rem(z + k, nz)))
    for j in range(1, peers):
        greet(plane_peer(j))
    for n in (nxt, prv):
        for c in range(n_core):
            greet({"sp": n, "tp": jnp.int32(c)})
    pl.semaphore_wait(barrier, nz - 1 + peers - 1 + 2 * n_core)

    edge = ci_hbm.shape[0] - HALO
    far = block + HALO
    partner = {"tp": other}
    swaps, halos = [], []
    for i, (src, dst) in enumerate(((ci_hbm, ci_f), (gi_hbm, gi_f))):
        halos.append(remote(src.at[pl.ds(edge, HALO)], dst.at[core, pl.ds(0, HALO)],
                            h_send.at[0, i], h_recv.at[core, i], {"sp": nxt, "tp": jnp.int32(0)}))
        halos.append(remote(src.at[pl.ds(0, HALO)], dst.at[core, pl.ds(far, HALO)],
                            h_send.at[1, i], h_recv.at[core, i], {"sp": prv, "tp": jnp.int32(1)}))
    notes = [
        remote(docs_hbm, docs.at[1], d_send.at[0], d_recv.at[0], {"sp": nxt, "tp": core}),
        remote(docs_hbm, docs.at[2], d_send.at[1], d_recv.at[1], {"sp": prv, "tp": core}),
    ]
    for i, (src, dst) in enumerate(((ci_hbm, ci_f), (gi_hbm, gi_f))):
        swaps.append(remote(src.at[pl.ds(theirs, span)], dst.at[core, pl.ds(their_at, span)],
                            e_send.at[i], e_recv.at[i], partner))
    swaps.append(remote(go_hbm.at[pl.ds(pl.multiple_of(other * block, HALO), block)], go_f.at[core],
                        e_send.at[2], e_recv.at[2], partner))
    swaps.append(remote(taps_hbm, taps_f.at[core], e_send.at[3], e_recv.at[3], partner))
    for copy in halos + notes + swaps:
        copy.start()
    lists = []
    for k in range(1, nz):
        to = at_z(lax.rem(z + k, nz))
        lists.append(remote(routes_hbm, rbuf.at[z], rt_send.at[k, 0], rt_recv.at[k, 0], to))
        lists.append(remote(rw_hbm, wbuf.at[z], rt_send.at[k, 1], rt_recv.at[k, 1], to))
    for copy in lists:
        copy.start()
    for load in weights:
        load.start()

    lane = lax.broadcasted_iota(jnp.int32, (block, block), 1)
    sub = lax.broadcasted_iota(jnp.int32, (block, block), 0)
    below = (sub < lane).astype(BF)

    def slots(k):
        b = ordered(k)
        chosen, weight = rbuf[b], wbuf[b]
        topk = chosen.shape[0]
        group = lax.broadcasted_iota(jnp.int32, (peers, block), 0)
        expert = z * peers + lax.rem(rank + group, peers)
        named = jnp.zeros((peers, block), F32)
        share = jnp.zeros((peers, block), F32)
        for i in range(topk):
            hit = jnp.broadcast_to(chosen[i:i + 1], (peers, block)) == expert
            named = jnp.where(hit, 1.0, named)
            share = jnp.where(hit, jnp.broadcast_to(weight[i:i + 1], (peers, block)), share)
        place = dot(named.astype(BF), below)
        place = jnp.where(named > 0.0, place, -1.0)
        seat = lax.broadcasted_iota(jnp.int32, (cap, block), 0).astype(F32)
        pieces = []
        for j in range(peers):
            here = jnp.broadcast_to(place[j:j + 1], (cap, block)) == seat
            select[k, j * cap:(j + 1) * cap, :] = jnp.where(here, 1.0, 0.0).astype(BF)
            pieces.append(jnp.where(here, jnp.broadcast_to(share[j:j + 1], (cap, block)), 0.0))
        spread[k] = jnp.concatenate(pieces, axis=0).T.astype(BF)

    for load in tables:
        load.wait()
    slots(0)

    for load in front:
        load.wait()
    for copy in notes + swaps:
        copy.wait_recv()
    for h in range(n_core):
        for i, dst in enumerate((ci_f, gi_f)):
            here = dst.at[h, pl.ds(pl.multiple_of(core * far, HALO), HALO)]
            remote(here, here, h_send.at[0, i], h_recv.at[h, i], partner).wait_recv()

    own, before_docs, after_docs = docs[0], docs[1], docs[2]
    first_half = core == 0
    wide = (8, block)

    def row(x):
        return jnp.broadcast_to(x.astype(F32), wide)

    cur = row(jnp.where(first_half, own[0:1], own[1:2]))
    left = row(jnp.where(first_half, before_docs[1:2], own[0:1]))
    right = row(jnp.where(first_half, own[1:2], after_docs[0:1]))
    lanes = lax.broadcasted_iota(jnp.int32, wide, 1)
    before = jnp.where(lanes == 0, pltpu.roll(left, 1, 1), pltpu.roll(cur, 1, 1))
    after = jnp.where(lanes == block - 1, pltpu.roll(right, block - 1, 1), pltpu.roll(cur, block - 1, 1))
    position = (me * n_core + core) * block + lanes
    has_before = (cur == before) & (position > 0)
    has_after = (cur == after) & (position < n_seq * n_core * block - 1)
    both = jnp.where(lax.broadcasted_iota(jnp.int32, wide, 0) == 0,
                     jnp.where(has_before, 1.0, 0.0), jnp.where(has_after, 1.0, 0.0))
    marks = jnp.concatenate([both] * (block // 8), axis=0).T
    keep_before, keep_after = marks[:, 0:1], marks[:, 1:2]

    for h in range(n_core):
        prod[...] = gi_f[h].astype(F32) * ci_f[h].astype(F32)
        conv = (
            taps_f[h, 0:1, :] * (prod[HALO - 1:HALO - 1 + block, :] * keep_before)
            + taps_f[h, 1:2, :] * prod[HALO:HALO + block, :]
            + taps_f[h, 2:3, :] * (prod[HALO + 1:HALO + 1 + block, :] * keep_after)
        )
        mixed[:, h * half:(h + 1) * half] = (go_f[h].astype(F32) * conv).astype(BF)

    project.wait()
    square = jnp.zeros((block, 128), F32)
    for q in range(nc):
        cols = slice(q * col, (q + 1) * col)
        value = stream[:, cols].astype(F32) + dot(mixed[...], wp[:, cols])
        hidden[:, cols] = value
        value = value * value
        for i in range(col // 128):
            square = square + value[:, i * 128:(i + 1) * 128]
    scale = lax.rsqrt(jnp.sum(square, axis=1, keepdims=True) / width + 1e-05)

    def chunk(q):
        return pl.ds(pl.multiple_of(q * col, col), col)

    def z_up(h, q):
        b = z - h
        piece = zbuf.at[b, :, chunk(q)]
        return remote(piece, piece, zu_send.at[h, q], z_recv.at[b, q], at_z(z + 1))

    def z_down(h, q):
        b = z + h
        piece = zbuf.at[b, :, chunk(q)]
        return remote(piece, piece, zd_send.at[h, q], z_recv.at[b, q], at_z(z - 1))

    for q in range(nc):
        cols = slice(q * col, (q + 1) * col)
        zbuf[z, :, cols] = (hidden[:, cols] * scale * gain[:, cols]).astype(BF)

    for q in range(nc):
        @pl.when(z < nz - 1)
        def _():
            z_up(0, q).start()

        @pl.when(z > 0)
        def _():
            z_down(0, q).start()

    def pump(h, q):
        @pl.when(z >= h)
        def _():
            piece = zbuf.at[z - h, :, chunk(q)]
            remote(piece, piece, zu_send.at[h, q], z_recv.at[z - h, q], at_z(z)).wait_recv()

            @pl.when(z < nz - 1)
            def _():
                z_up(h, q).start()

        @pl.when(z + h < nz)
        def _():
            piece = zbuf.at[z + h, :, chunk(q)]
            remote(piece, piece, zd_send.at[h, q], z_recv.at[z + h, q], at_z(z)).wait_recv()

            @pl.when(z > 0)
            def _():
                z_down(h, q).start()

    def a_copy(k, j, q):
        return remote(
            outgoing.at[k, pl.ds((j - 1) * cap, cap), chunk(q)], arrived.at[k, pl.ds(j * cap, cap), chunk(q)],
            a_send.at[k, q], a_recv.at[k, q], plane_peer(j))

    def a_all(k, q):
        return remote(outgoing.at[k, :, chunk(q)], arrived.at[k, pl.ds(cap, rows - cap), chunk(q)],
                      a_send.at[k, q], a_recv.at[k, q], plane_peer(1))

    def r_copy(k, j, q):
        return remote(
            arrived.at[k, pl.ds(j * cap, cap), chunk(q)], returned.at[k, pl.ds(j * cap, cap), chunk(q)],
            r_send.at[k, q], r_recv.at[k, q], plane_peer(peers - j))

    def r_all(k, q):
        return remote(
            arrived.at[k, pl.ds(cap, rows - cap), chunk(q)], returned.at[k, pl.ds(cap, rows - cap), chunk(q)],
            r_send.at[k, q], r_recv.at[k, q], plane_peer(1))

    def dispatch(k):
        b = ordered(k)

        @pl.loop(0, nc)
        def _(q):
            if k:
                pump(k, q)
            cols = chunk(q)
            picked = dot(select[k], zbuf[b, :, cols]).astype(BF)
            arrived[k, 0:cap, cols] = picked[:cap]
            outgoing[k, :, cols] = picked[cap:]
            for j in range(1, peers):
                a_copy(k, j, q).start()

    fcol = tile_of(ff, 256)

    def expert(k):
        if k == 0:
            for load in weights:
                load.wait()

        @pl.loop(0, nc)
        def _(q):
            a_all(k, q).wait_recv()

        @pl.loop(0, ff // fcol)
        def _(i):
            cols = pl.ds(pl.multiple_of(i * fcol, fcol), fcol)
            gate = jnp.minimum(dot(arrived[k], wg[:, cols]), 7.0)
            upper = jnp.clip(dot(arrived[k], wu[:, cols]), -7.0, 7.0)
            act[:, cols] = ((upper + 1.0) * gate * jax.nn.sigmoid(1.702 * gate)).astype(BF)

        @pl.loop(0, nc)
        def _(q):
            cols = chunk(q)
            res = dot(act[...], wd[:, cols]).astype(BF)
            returned[k, 0:cap, cols] = res[:cap]
            arrived[k, cap:, cols] = res[cap:]
            if k:
                give(k, q)

    def give(k, q):
        for j in range(1, peers):
            r_copy(k, j, q).start()

    def p_copy(k, q):
        b = ordered(k)
        return remote(
            partial.at[k - 1, :, chunk(q)], summed.at[lax.rem(z - b + nz, nz) - 1, :, chunk(q)],
            p_send.at[k, q], p_recv.at[q], at_z(b))

    def combine(k):
        @pl.loop(0, nc)
        def _(q):
            cols = chunk(q)
            r_all(k, q).wait_recv()
            total = dot(spread[k], returned[k, :, cols])
            if k == 0:
                hidden[:, cols] = hidden[:, cols] + total
            else:
                partial[k - 1, :, cols] = total.astype(BF)
                p_copy(k, q).start()

    dispatch(0)
    for copy in lists:
        copy.wait_recv()
    for k in range(1, nz):
        slots(k)
        dispatch(k)
        expert(k - 1)
        if k >= 3:
            combine(k - 2)
    expert(nz - 1)

    @pl.loop(0, nc)
    def _(q):
        give(0, q)

    for k in range(max(1, nz - 2), nz):
        combine(k)
    combine(0)

    for q in range(nc):
        piece = summed.at[:, :, chunk(q)]
        remote(piece, piece, p_send.at[0, q], p_recv.at[q], at_z(z)).wait_recv()
        cols = slice(q * col, (q + 1) * col)
        total = hidden[:, cols]
        for i in range(nz - 1):
            total = total + summed[i, :, cols].astype(F32)
        out_ref[:, cols] = total.astype(BF)

    for copy in halos + notes + swaps + lists:
        copy.wait_send()

    @pl.loop(0, nc)
    def _(q):
        for h in range(nz):
            @pl.when((z >= h) & (z < nz - 1))
            def _():
                z_up(h, q).wait_send()

            @pl.when((z + h < nz) & (z > 0))
            def _():
                z_down(h, q).wait_send()
        for k in range(nz):
            a_all(k, q).wait_send()
            r_all(k, q).wait_send()
            if k:
                p_copy(k, q).wait_send()


def layer(n_seq, nz, n_plane, n_core, cap, *args):
    tok, half = args[0].shape
    block, width = args[6].shape
    ff = args[10].shape[1]
    peers = n_plane * n_core
    rows = peers * cap
    topk = args[8].shape[0]
    channels = half * n_core
    frame = block + 2 * HALO
    col = tile_of(width, 512)
    nc = width // col
    hbm = pl.BlockSpec(memory_space=pl.ANY)
    vmem = pl.BlockSpec(memory_space=pltpu.VMEM)
    dma = pltpu.SemaphoreType.DMA
    return pl.pallas_call(
        functools.partial(layer_kernel, n_seq, nz, n_plane, n_core, cap, col),
        out_shape=jax.ShapeDtypeStruct((block, width), BF),
        in_specs=[hbm] * len(args),
        out_specs=vmem,
        scratch_shapes=[
            pltpu.VMEM((width, ff), BF),
            pltpu.VMEM((width, ff), BF),
            pltpu.VMEM((ff, width), BF),
            pltpu.VMEM((channels, width), BF),
            pltpu.VMEM((n_core, frame, half), BF),
            pltpu.VMEM((n_core, frame, half), BF),
            pltpu.VMEM((n_core, block, half), BF),
            pltpu.VMEM((n_core,) + args[3].shape, F32),
            pltpu.VMEM((3, n_core, block), jnp.int32),
            pltpu.VMEM((frame, half), F32),
            pltpu.VMEM((block, channels), BF),
            pltpu.VMEM((block, width), BF),
            pltpu.VMEM((1, width), F32),
            pltpu.VMEM((block, width), F32),
            pltpu.VMEM((nz, topk, block), jnp.int32),
            pltpu.VMEM((nz, topk, block), F32),
            pltpu.VMEM((nz, rows, block), BF),
            pltpu.VMEM((nz, block, rows), BF),
            pltpu.VMEM((nz, block, width), BF),
            pltpu.VMEM((nz, rows - cap, width), BF),
            pltpu.VMEM((nz, rows, width), BF),
            pltpu.VMEM((rows, ff), BF),
            pltpu.VMEM((nz, rows, width), BF),
            pltpu.VMEM((nz - 1, block, width), BF),
            pltpu.VMEM((nz - 1, block, width), BF),
            dma((13,)), dma((4,)), dma((4,)), dma((2, 2)), dma((n_core, 2)),
            dma((2,)), dma((2,)), dma((nz, 2)), dma((nz, 2)),
            dma((nz, nc)), dma((nz, nc)), dma((nz, nc)),
            dma((nz, nc)), dma((nz, nc)), dma((nz, nc)), dma((nz, nc)),
            dma((nz, nc)), dma((nc,)),
        ],
        compiler_params=pltpu.CompilerParams(
            collective_id=0, has_side_effects=True, vmem_limit_bytes=62 * 2**20),
        name="mixer_experts",
    )(*args)


def per_device(
    conv_in, gate_outer, gate_inner, tap_weights, doc_ids, w_proj, stream, norm_gain,
    routes, route_weights, w_gate, w_up, w_down,
):
    n_seq = lax.axis_size("sp")
    n_core = lax.axis_size("tp")
    tok_dev = conv_in.shape[0]
    topk = routes.shape[1]
    capacity = max(2, 2 * tok_dev * topk // (n_core * n_seq * n_core))
    capacity = -(-capacity // 16) * 16
    nz = max(d for d in range(1, math.isqrt(n_seq) + 1) if n_seq % d == 0)
    return layer(
        n_seq, nz, n_seq // nz, n_core, capacity,
        conv_in, gate_outer, gate_inner, tap_weights,
        doc_ids.reshape(n_core, tok_dev // n_core), w_proj, stream, norm_gain.reshape(1, -1),
        routes.T, route_weights.T, w_gate[0], w_up[0], w_down[0])


def solution(mesh):
    in_specs = (
        P("sp", "tp"),
        P("sp", "tp"),
        P("sp", "tp"),
        P(None, "tp"),
        P("sp"),
        P(),
        P(("sp", "tp"), None),
        P(),
        P(("sp", "tp"), None),
        P(("sp", "tp"), None),
        P(("sp", "tp"), None, None),
        P(("sp", "tp"), None, None),
        P(("sp", "tp"), None, None),
    )
    return jax.shard_map(
        per_device, mesh=mesh, in_specs=in_specs, out_specs=P(("sp", "tp"), None), check_vma=False
    )
```

```python
import functools
import math

import jax
import jax.numpy as jnp
from jax import lax
from jax.experimental import pallas as pl
from jax.experimental.pallas import tpu as pltpu
from jax.sharding import PartitionSpec as P

MESH = pl.DeviceIdType.MESH
HALO = 16
BF = jnp.bfloat16
F32 = jnp.float32


def dot(a, b):
    return jnp.dot(a, b, preferred_element_type=F32)


def tile_of(size, most):
    return next(t for t in range(most, 0, -128) if size % t == 0)


def nearest_first(nz):
    return [sorted(range(nz), key=lambda b: (abs(b - z), abs(2 * b - nz + 1) * (1 if nz > 2 else 0), b))
            for z in range(nz)]


def layer_kernel(
    n_seq, nz, n_plane, n_core, cap, col,
    ci_hbm, go_hbm, gi_hbm, taps_hbm, docs_hbm, wp_hbm, stream_hbm, gain_hbm,
    routes_hbm, rw_hbm, wg_hbm, wu_hbm, wd_hbm,
    out_ref,
    wg, wu, wd, wp, ci_f, gi_f, go_f, taps_f, docs, prod, mixed, stream, gain, hidden,
    rbuf, wbuf, select, spread, zbuf, outgoing, arrived, act, returned, partial, chain,
    l_sem, e_send, e_recv, h_send, h_recv, d_send, d_recv, rt_send, rt_recv,
    zu_send, zd_send, z_recv, a_send, a_recv, r_send, r_recv, p_send, p_recv,
):
    peers = n_plane * n_core
    rows = peers * cap
    block, width = hidden.shape
    ff = wg.shape[1]
    half = ci_hbm.shape[1]
    span = block + HALO
    nc = width // col
    me = lax.axis_index("sp")
    core = lax.axis_index("tp")
    z, p = me // n_plane, lax.rem(me, n_plane)
    rank = p * n_core + core
    other = 1 - core

    def at_z(b):
        return {"sp": b * n_plane + p, "tp": core}

    def plane_peer(j):
        q = lax.rem(rank + j, peers)
        return {"sp": z * n_plane + q // n_core, "tp": lax.rem(q, n_core)}

    nxt, prv = lax.rem(me + 1, n_seq), lax.rem(me + n_seq - 1, n_seq)
    order = nearest_first(nz)

    def ordered(k):
        total = jnp.int32(0)
        for i in range(nz):
            total = total + jnp.where(z == i, order[i][k], 0)
        return total

    def remote(src, dst, send, recv, to):
        return pltpu.make_async_remote_copy(
            src_ref=src, dst_ref=dst, send_sem=send, recv_sem=recv,
            device_id=to, device_id_type=MESH)

    mine = pl.multiple_of(core * (block - HALO), HALO)
    theirs = pl.multiple_of(other * (block - HALO), HALO)
    my_at = pl.multiple_of(other * HALO, HALO)
    their_at = pl.multiple_of(core * HALO, HALO)

    def local(i, src, dst):
        return pltpu.make_async_copy(src, dst, l_sem.at[i])

    front = [
        local(0, ci_hbm.at[pl.ds(mine, span)], ci_f.at[core, pl.ds(my_at, span)]),
        local(1, gi_hbm.at[pl.ds(mine, span)], gi_f.at[core, pl.ds(my_at, span)]),
        local(2, go_hbm.at[pl.ds(pl.multiple_of(core * block, HALO), block)], go_f.at[core]),
        local(3, taps_hbm, taps_f.at[core]),
        local(4, docs_hbm, docs.at[0]),
        local(5, stream_hbm, stream),
        local(6, gain_hbm, gain),
    ]
    tables = [local(7, routes_hbm, rbuf.at[z]), local(8, rw_hbm, wbuf.at[z])]
    project = local(9, wp_hbm, wp)
    weights = [local(10, wg_hbm, wg), local(11, wu_hbm, wu), local(12, wd_hbm, wd)]
    for load in front + tables + [project] + weights:
        load.start()

    barrier = pltpu.get_barrier_semaphore()

    def greet(to):
        pl.semaphore_signal(barrier, inc=1, device_id=to, device_id_type=MESH)

    for k in range(1, nz):
        greet(at_z(lax.rem(z + k, nz)))
    for j in range(1, peers):
        greet(plane_peer(j))
    for n in (nxt, prv):
        for c in range(n_core):
            greet({"sp": n, "tp": jnp.int32(c)})
    pl.semaphore_wait(barrier, nz - 1 + peers - 1 + 2 * n_core)

    edge = ci_hbm.shape[0] - HALO
    far = block + HALO
    partner = {"tp": other}
    swaps, halos = [], []
    for i, (src, dst) in enumerate(((ci_hbm, ci_f), (gi_hbm, gi_f))):
        halos.append(remote(src.at[pl.ds(edge, HALO)], dst.at[core, pl.ds(0, HALO)],
                            h_send.at[0, i], h_recv.at[core, i], {"sp": nxt, "tp": jnp.int32(0)}))
        halos.append(remote(src.at[pl.ds(0, HALO)], dst.at[core, pl.ds(far, HALO)],
                            h_send.at[1, i], h_recv.at[core, i], {"sp": prv, "tp": jnp.int32(1)}))
    notes = [
        remote(docs_hbm, docs.at[1], d_send.at[0], d_recv.at[0], {"sp": nxt, "tp": core}),
        remote(docs_hbm, docs.at[2], d_send.at[1], d_recv.at[1], {"sp": prv, "tp": core}),
    ]
    for i, (src, dst) in enumerate(((ci_hbm, ci_f), (gi_hbm, gi_f))):
        swaps.append(remote(src.at[pl.ds(theirs, span)], dst.at[core, pl.ds(their_at, span)],
                            e_send.at[i], e_recv.at[i], partner))
    swaps.append(remote(go_hbm.at[pl.ds(pl.multiple_of(other * block, HALO), block)], go_f.at[core],
                        e_send.at[2], e_recv.at[2], partner))
    swaps.append(remote(taps_hbm, taps_f.at[core], e_send.at[3], e_recv.at[3], partner))
    for copy in halos + notes + swaps:
        copy.start()
    lists = []
    for k in range(1, nz):
        to = at_z(lax.rem(z + k, nz))
        lists.append(remote(routes_hbm, rbuf.at[z], rt_send.at[k, 0], rt_recv.at[k, 0], to))
        lists.append(remote(rw_hbm, wbuf.at[z], rt_send.at[k, 1], rt_recv.at[k, 1], to))
    for copy in lists:
        copy.start()

    lane = lax.broadcasted_iota(jnp.int32, (block, block), 1)
    sub = lax.broadcasted_iota(jnp.int32, (block, block), 0)
    below = (sub < lane).astype(BF)

    def slots(k):
        b = ordered(k)
        chosen, weight = rbuf[b], wbuf[b]
        topk = chosen.shape[0]
        group = lax.broadcasted_iota(jnp.int32, (peers, block), 0)
        expert = z * peers + lax.rem(rank + group, peers)
        named = jnp.zeros((peers, block), F32)
        share = jnp.zeros((peers, block), F32)
        for i in range(topk):
            hit = jnp.broadcast_to(chosen[i:i + 1], (peers, block)) == expert
            named = jnp.where(hit, 1.0, named)
            share = jnp.where(hit, jnp.broadcast_to(weight[i:i + 1], (peers, block)), share)
        place = dot(named.astype(BF), below)
        place = jnp.where(named > 0.0, place, -1.0)
        seat = lax.broadcasted_iota(jnp.int32, (cap, block), 0).astype(F32)
        pieces = []
        for j in range(peers):
            here = jnp.broadcast_to(place[j:j + 1], (cap, block)) == seat
            select[k, j * cap:(j + 1) * cap, :] = jnp.where(here, 1.0, 0.0).astype(BF)
            pieces.append(jnp.where(here, jnp.broadcast_to(share[j:j + 1], (cap, block)), 0.0))
        spread[k] = jnp.concatenate(pieces, axis=0).T.astype(BF)

    for load in tables:
        load.wait()
    slots(0)

    for load in front:
        load.wait()
    for copy in notes + swaps:
        copy.wait_recv()
    for h in range(n_core):
        for i, dst in enumerate((ci_f, gi_f)):
            here = dst.at[h, pl.ds(pl.multiple_of(core * far, HALO), HALO)]
            remote(here, here, h_send.at[0, i], h_recv.at[h, i], partner).wait_recv()

    own, before_docs, after_docs = docs[0], docs[1], docs[2]
    first_half = core == 0
    wide = (8, block)

    def row(x):
        return jnp.broadcast_to(x.astype(F32), wide)

    cur = row(jnp.where(first_half, own[0:1], own[1:2]))
    left = row(jnp.where(first_half, before_docs[1:2], own[0:1]))
    right = row(jnp.where(first_half, own[1:2], after_docs[0:1]))
    lanes = lax.broadcasted_iota(jnp.int32, wide, 1)
    before = jnp.where(lanes == 0, pltpu.roll(left, 1, 1), pltpu.roll(cur, 1, 1))
    after = jnp.where(lanes == block - 1, pltpu.roll(right, block - 1, 1), pltpu.roll(cur, block - 1, 1))
    position = (me * n_core + core) * block + lanes
    has_before = (cur == before) & (position > 0)
    has_after = (cur == after) & (position < n_seq * n_core * block - 1)
    both = jnp.where(lax.broadcasted_iota(jnp.int32, wide, 0) == 0,
                     jnp.where(has_before, 1.0, 0.0), jnp.where(has_after, 1.0, 0.0))
    marks = jnp.concatenate([both] * (block // 8), axis=0).T
    keep_before, keep_after = marks[:, 0:1], marks[:, 1:2]

    for h in range(n_core):
        prod[...] = gi_f[h].astype(F32) * ci_f[h].astype(F32)
        conv = (
            taps_f[h, 0:1, :] * (prod[HALO - 1:HALO - 1 + block, :] * keep_before)
            + taps_f[h, 1:2, :] * prod[HALO:HALO + block, :]
            + taps_f[h, 2:3, :] * (prod[HALO + 1:HALO + 1 + block, :] * keep_after)
        )
        mixed[:, h * half:(h + 1) * half] = (go_f[h].astype(F32) * conv).astype(BF)

    project.wait()
    square = jnp.zeros((block, 128), F32)
    for q in range(nc):
        cols = slice(q * col, (q + 1) * col)
        value = stream[:, cols].astype(F32) + dot(mixed[...], wp[:, cols])
        hidden[:, cols] = value
        value = value * value
        for i in range(col // 128):
            square = square + value[:, i * 128:(i + 1) * 128]
    scale = lax.rsqrt(jnp.sum(square, axis=1, keepdims=True) / width + 1e-05)

    def chunk(q):
        return pl.ds(pl.multiple_of(q * col, col), col)

    def z_up(h, q):
        b = z - h
        piece = zbuf.at[b, :, chunk(q)]
        return remote(piece, piece, zu_send.at[h, q], z_recv.at[b, q], at_z(z + 1))

    def z_down(h, q):
        b = z + h
        piece = zbuf.at[b, :, chunk(q)]
        return remote(piece, piece, zd_send.at[h, q], z_recv.at[b, q], at_z(z - 1))

    for q in range(nc):
        cols = slice(q * col, (q + 1) * col)
        zbuf[z, :, cols] = (hidden[:, cols] * scale * gain[:, cols]).astype(BF)

    for q in range(nc):
        @pl.when(z < nz - 1)
        def _():
            z_up(0, q).start()

        @pl.when(z > 0)
        def _():
            z_down(0, q).start()

    def pump(h, q):
        @pl.when(z >= h)
        def _():
            piece = zbuf.at[z - h, :, chunk(q)]
            remote(piece, piece, zu_send.at[h, q], z_recv.at[z - h, q], at_z(z)).wait_recv()

            @pl.when(z < nz - 1)
            def _():
                z_up(h, q).start()

        @pl.when(z + h < nz)
        def _():
            piece = zbuf.at[z + h, :, chunk(q)]
            remote(piece, piece, zd_send.at[h, q], z_recv.at[z + h, q], at_z(z)).wait_recv()

            @pl.when(z > 0)
            def _():
                z_down(h, q).start()

    def a_copy(k, j, q):
        return remote(
            outgoing.at[k, pl.ds((j - 1) * cap, cap), chunk(q)], arrived.at[k, pl.ds(j * cap, cap), chunk(q)],
            a_send.at[k, q], a_recv.at[k, q], plane_peer(j))

    def a_all(k, q):
        return remote(outgoing.at[k, :, chunk(q)], arrived.at[k, pl.ds(cap, rows - cap), chunk(q)],
                      a_send.at[k, q], a_recv.at[k, q], plane_peer(1))

    def r_copy(k, j, q):
        return remote(
            arrived.at[k, pl.ds(j * cap, cap), chunk(q)], returned.at[k, pl.ds(j * cap, cap), chunk(q)],
            r_send.at[k, q], r_recv.at[k, q], plane_peer(peers - j))

    def r_all(k, q):
        return remote(
            arrived.at[k, pl.ds(cap, rows - cap), chunk(q)], returned.at[k, pl.ds(cap, rows - cap), chunk(q)],
            r_send.at[k, q], r_recv.at[k, q], plane_peer(1))

    def dispatch(k):
        b = ordered(k)

        @pl.loop(0, nc)
        def _(q):
            if k:
                pump(k, q)
            cols = chunk(q)
            picked = dot(select[k], zbuf[b, :, cols]).astype(BF)
            arrived[k, 0:cap, cols] = picked[:cap]
            outgoing[k, :, cols] = picked[cap:]
            for j in range(1, peers):
                a_copy(k, j, q).start()

    fcol = tile_of(ff, 256)

    def expert(k):
        if k == 0:
            for load in weights:
                load.wait()

        @pl.loop(0, nc)
        def _(q):
            a_all(k, q).wait_recv()

        @pl.loop(0, ff // fcol)
        def _(i):
            cols = pl.ds(pl.multiple_of(i * fcol, fcol), fcol)
            gate = jnp.minimum(dot(arrived[k], wg[:, cols]), 7.0)
            upper = jnp.clip(dot(arrived[k], wu[:, cols]), -7.0, 7.0)
            act[:, cols] = ((upper + 1.0) * gate * jax.nn.sigmoid(1.702 * gate)).astype(BF)

        @pl.loop(0, nc)
        def _(q):
            cols = chunk(q)
            res = dot(act[...], wd[:, cols]).astype(BF)
            returned[k, 0:cap, cols] = res[:cap]
            arrived[k, cap:, cols] = res[cap:]
            if k == nz - 1:
                give(k, q)

    def give(k, q):
        for j in range(1, peers):
            r_copy(k, j, q).start()

    def chained(b):
        return ((b < z) & (z < nz - 1)) | ((b > z) & (z > 0))

    def p_copy(k, q):
        b = ordered(k)
        down = b < z
        seat = jnp.where(down & (b == z - 1), nz, b)
        return remote(partial.at[k - 1, :, chunk(q)], chain.at[seat, :, chunk(q)],
                      p_send.at[k, q], p_recv.at[seat, q], at_z(jnp.where(down, z - 1, z + 1)))

    def p_wait(seat, q):
        piece = chain.at[seat, :, chunk(q)]
        remote(piece, piece, p_send.at[0, q], p_recv.at[seat, q], at_z(z)).wait_recv()

    def combine(k):
        b = ordered(k)

        @pl.loop(0, nc)
        def _(q):
            cols = chunk(q)
            r_all(k, q).wait_recv()
            total = dot(spread[k], returned[k, :, cols])
            if k == 0:
                hidden[:, cols] = hidden[:, cols] + total
            else:
                @pl.when(chained(b))
                def _():
                    p_wait(b, q)
                    partial[k - 1, :, cols] = (total + chain[b, :, cols].astype(F32)).astype(BF)

                @pl.when(jnp.logical_not(chained(b)))
                def _():
                    partial[k - 1, :, cols] = total.astype(BF)

                p_copy(k, q).start()

    dispatch(0)
    for copy in lists:
        copy.wait_recv()
    for k in range(1, nz):
        slots(k)
        dispatch(k)
        if k < nz - 1:
            expert(k - 1)

    def give_all(k, low, high):
        @pl.loop(low, high)
        def _(q):
            give(k, q)

    give_all(0, 0, nc // 2)
    expert(nz - 2)
    expert(nz - 1)
    for k in range(nz - 2, 0, -1):
        give_all(k, 0, nc)
    give_all(0, nc // 2, nc)
    for k in range(nz - 1, -1, -1):
        combine(k)

    @pl.loop(0, nc)
    def _(q):
        cols = chunk(q)

        @pl.when(z > 0)
        def _():
            p_wait(z, q)
            hidden[:, cols] = hidden[:, cols] + chain[z, :, cols].astype(F32)

        @pl.when(z < nz - 1)
        def _():
            p_wait(nz, q)
            hidden[:, cols] = hidden[:, cols] + chain[nz, :, cols].astype(F32)

        out_ref[:, cols] = hidden[:, cols].astype(BF)

    for copy in halos + notes + swaps + lists:
        copy.wait_send()

    @pl.loop(0, nc)
    def _(q):
        for h in range(nz):
            @pl.when((z >= h) & (z < nz - 1))
            def _():
                z_up(h, q).wait_send()

            @pl.when((z + h < nz) & (z > 0))
            def _():
                z_down(h, q).wait_send()
        for k in range(nz):
            a_all(k, q).wait_send()
            r_all(k, q).wait_send()
            if k:
                p_copy(k, q).wait_send()


def layer(n_seq, nz, n_plane, n_core, cap, *args):
    tok, half = args[0].shape
    block, width = args[6].shape
    ff = args[10].shape[1]
    peers = n_plane * n_core
    rows = peers * cap
    topk = args[8].shape[0]
    channels = half * n_core
    frame = block + 2 * HALO
    col = tile_of(width, 512)
    nc = width // col
    hbm = pl.BlockSpec(memory_space=pl.ANY)
    vmem = pl.BlockSpec(memory_space=pltpu.VMEM)
    dma = pltpu.SemaphoreType.DMA
    return pl.pallas_call(
        functools.partial(layer_kernel, n_seq, nz, n_plane, n_core, cap, col),
        out_shape=jax.ShapeDtypeStruct((block, width), BF),
        in_specs=[hbm] * len(args),
        out_specs=vmem,
        scratch_shapes=[
            pltpu.VMEM((width, ff), BF),
            pltpu.VMEM((width, ff), BF),
            pltpu.VMEM((ff, width), BF),
            pltpu.VMEM((channels, width), BF),
            pltpu.VMEM((n_core, frame, half), BF),
            pltpu.VMEM((n_core, frame, half), BF),
            pltpu.VMEM((n_core, block, half), BF),
            pltpu.VMEM((n_core,) + args[3].shape, F32),
            pltpu.VMEM((3, n_core, block), jnp.int32),
            pltpu.VMEM((frame, half), F32),
            pltpu.VMEM((block, channels), BF),
            pltpu.VMEM((block, width), BF),
            pltpu.VMEM((1, width), F32),
            pltpu.VMEM((block, width), F32),
            pltpu.VMEM((nz, topk, block), jnp.int32),
            pltpu.VMEM((nz, topk, block), F32),
            pltpu.VMEM((nz, rows, block), BF),
            pltpu.VMEM((nz, block, rows), BF),
            pltpu.VMEM((nz, block, width), BF),
            pltpu.VMEM((nz, rows - cap, width), BF),
            pltpu.VMEM((nz, rows, width), BF),
            pltpu.VMEM((rows, ff), BF),
            pltpu.VMEM((nz, rows, width), BF),
            pltpu.VMEM((nz - 1, block, width), BF),
            pltpu.VMEM((nz + 1, block, width), BF),
            dma((13,)), dma((4,)), dma((4,)), dma((2, 2)), dma((n_core, 2)),
            dma((2,)), dma((2,)), dma((nz, 2)), dma((nz, 2)),
            dma((nz, nc)), dma((nz, nc)), dma((nz, nc)),
            dma((nz, nc)), dma((nz, nc)), dma((nz, nc)), dma((nz, nc)),
            dma((nz, nc)), dma((nz + 1, nc)),
        ],
        compiler_params=pltpu.CompilerParams(
            collective_id=0, has_side_effects=True, vmem_limit_bytes=62 * 2**20),
        name="mixer_experts",
    )(*args)


def per_device(
    conv_in, gate_outer, gate_inner, tap_weights, doc_ids, w_proj, stream, norm_gain,
    routes, route_weights, w_gate, w_up, w_down,
):
    n_seq = lax.axis_size("sp")
    n_core = lax.axis_size("tp")
    tok_dev = conv_in.shape[0]
    topk = routes.shape[1]
    capacity = max(2, 2 * tok_dev * topk // (n_core * n_seq * n_core))
    capacity = -(-capacity // 16) * 16
    nz = max(d for d in range(1, math.isqrt(n_seq) + 1) if n_seq % d == 0)
    return layer(
        n_seq, nz, n_seq // nz, n_core, capacity,
        conv_in, gate_outer, gate_inner, tap_weights,
        doc_ids.reshape(n_core, tok_dev // n_core), w_proj, stream, norm_gain.reshape(1, -1),
        routes.T, route_weights.T, w_gate[0], w_up[0], w_down[0])


def solution(mesh):
    in_specs = (
        P("sp", "tp"),
        P("sp", "tp"),
        P("sp", "tp"),
        P(None, "tp"),
        P("sp"),
        P(),
        P(("sp", "tp"), None),
        P(),
        P(("sp", "tp"), None),
        P(("sp", "tp"), None),
        P(("sp", "tp"), None, None),
        P(("sp", "tp"), None, None),
        P(("sp", "tp"), None, None),
    )
    return jax.shard_map(
        per_device, mesh=mesh, in_specs=in_specs, out_specs=P(("sp", "tp"), None), check_vma=False
    )
```

```python
import functools
import math

import jax
import jax.numpy as jnp
from jax import lax
from jax.experimental import pallas as pl
from jax.experimental.pallas import tpu as pltpu
from jax.sharding import PartitionSpec as P

MESH = pl.DeviceIdType.MESH
HALO = 16
SLAB = 256
COL = 896
BF = jnp.bfloat16
F32 = jnp.float32


def dot(a, b):
    return jnp.dot(a, b, preferred_element_type=F32)


def tile_of(size, most):
    return next(t for t in range(most, 0, -128) if size % t == 0)


def nearest_first(nz):
    return [sorted(range(nz), key=lambda b: (abs(b - z), abs(2 * b - nz + 1) * (1 if nz > 2 else 0), b))
            for z in range(nz)]


def layer_kernel(
    n_seq, nz, n_plane, n_core, cap, col, slab,
    ci_hbm, go_hbm, gi_hbm, taps_hbm, docs_hbm, wp_hbm, stream_hbm, gain_hbm,
    routes_hbm, rw_hbm, wg_hbm, wu_hbm, wd_hbm,
    out_ref,
    wg, wu, wd, wp, ci_f, gi_f, go_f, taps_f, docs, prod, mixed, stream, gain, hidden,
    rbuf, wbuf, select, spread, zbuf, outgoing, arrived, act, returned, partial, chain,
    rbuf2, wbuf2, select2, spread2, pslab, outgoing2, returned2, partial2, summed2,
    l_sem, e_send, e_recv, h_send, h_recv, d_send, d_recv, rt_send, rt_recv,
    zu_send, zd_send, z_recv, a_send, a_recv, r_send, r_recv, p_send, p_recv,
    rt2_send, rt2_recv, s_send, s_recv, v_send, v_recv, w_send, w_recv, f_send, f_recv,
):
    peers = n_plane * n_core
    rows = peers * cap
    block, width = hidden.shape
    ff = wg.shape[1]
    half = ci_hbm.shape[1]
    span = block + HALO
    main = width - slab
    nc = main // col
    wide_col = tile_of(width, 512)
    me = lax.axis_index("sp")
    core = lax.axis_index("tp")
    z, p = me // n_plane, lax.rem(me, n_plane)
    rank = p * n_core + core
    other = 1 - core

    def at_z(b):
        return {"sp": b * n_plane + p, "tp": core}

    def in_plane(q):
        return {"sp": z * n_plane + q, "tp": core}

    def plane_peer(j):
        q = lax.rem(rank + j, peers)
        return {"sp": z * n_plane + q // n_core, "tp": lax.rem(q, n_core)}

    nxt, prv = lax.rem(me + 1, n_seq), lax.rem(me + n_seq - 1, n_seq)
    order = nearest_first(nz)

    def ordered(k):
        total = jnp.int32(0)
        for i in range(nz):
            total = total + jnp.where(z == i, order[i][k], 0)
        return total

    def remote(src, dst, send, recv, to):
        return pltpu.make_async_remote_copy(
            src_ref=src, dst_ref=dst, send_sem=send, recv_sem=recv,
            device_id=to, device_id_type=MESH)

    mine = pl.multiple_of(core * (block - HALO), HALO)
    theirs = pl.multiple_of(other * (block - HALO), HALO)
    my_at = pl.multiple_of(other * HALO, HALO)
    their_at = pl.multiple_of(core * HALO, HALO)

    def local(i, src, dst):
        return pltpu.make_async_copy(src, dst, l_sem.at[i])

    front = [
        local(0, ci_hbm.at[pl.ds(mine, span)], ci_f.at[core, pl.ds(my_at, span)]),
        local(1, gi_hbm.at[pl.ds(mine, span)], gi_f.at[core, pl.ds(my_at, span)]),
        local(2, go_hbm.at[pl.ds(pl.multiple_of(core * block, HALO), block)], go_f.at[core]),
        local(3, taps_hbm, taps_f.at[core]),
        local(4, docs_hbm, docs.at[0]),
        local(5, stream_hbm, stream),
        local(6, gain_hbm, gain),
    ]
    tables = [local(7, routes_hbm, rbuf.at[z]), local(8, rw_hbm, wbuf.at[z]),
              local(13, routes_hbm, rbuf2.at[p]), local(14, rw_hbm, wbuf2.at[p])]
    project = local(9, wp_hbm, wp)
    weights = [local(10, wg_hbm, wg), local(11, wu_hbm, wu), local(12, wd_hbm, wd)]
    for load in front + tables + [project] + weights:
        load.start()

    barrier = pltpu.get_barrier_semaphore()

    def greet(to):
        pl.semaphore_signal(barrier, inc=1, device_id=to, device_id_type=MESH)

    for k in range(1, nz):
        greet(at_z(lax.rem(z + k, nz)))
        greet({"sp": lax.rem(z + k, nz) * n_plane + p, "tp": other})
    for j in range(1, peers):
        greet(plane_peer(j))
    for n in (nxt, prv):
        for c in range(n_core):
            greet({"sp": n, "tp": jnp.int32(c)})
    pl.semaphore_wait(barrier, 2 * (nz - 1) + peers - 1 + 2 * n_core)

    edge = ci_hbm.shape[0] - HALO
    far = block + HALO
    partner = {"tp": other}
    swaps, halos = [], []
    for i, (src, dst) in enumerate(((ci_hbm, ci_f), (gi_hbm, gi_f))):
        halos.append(remote(src.at[pl.ds(edge, HALO)], dst.at[core, pl.ds(0, HALO)],
                            h_send.at[0, i], h_recv.at[core, i], {"sp": nxt, "tp": jnp.int32(0)}))
        halos.append(remote(src.at[pl.ds(0, HALO)], dst.at[core, pl.ds(far, HALO)],
                            h_send.at[1, i], h_recv.at[core, i], {"sp": prv, "tp": jnp.int32(1)}))
    notes = [
        remote(docs_hbm, docs.at[1], d_send.at[0], d_recv.at[0], {"sp": nxt, "tp": core}),
        remote(docs_hbm, docs.at[2], d_send.at[1], d_recv.at[1], {"sp": prv, "tp": core}),
    ]
    for i, (src, dst) in enumerate(((ci_hbm, ci_f), (gi_hbm, gi_f))):
        swaps.append(remote(src.at[pl.ds(theirs, span)], dst.at[core, pl.ds(their_at, span)],
                            e_send.at[i], e_recv.at[i], partner))
    swaps.append(remote(go_hbm.at[pl.ds(pl.multiple_of(other * block, HALO), block)], go_f.at[core],
                        e_send.at[2], e_recv.at[2], partner))
    swaps.append(remote(taps_hbm, taps_f.at[core], e_send.at[3], e_recv.at[3], partner))
    for copy in halos + notes + swaps:
        copy.start()
    lists = []
    for k in range(1, nz):
        to = at_z(lax.rem(z + k, nz))
        lists.append(remote(routes_hbm, rbuf.at[z], rt_send.at[k, 0], rt_recv.at[k, 0], to))
        lists.append(remote(rw_hbm, wbuf.at[z], rt_send.at[k, 1], rt_recv.at[k, 1], to))
    for i in range(1, n_plane):
        to = in_plane(lax.rem(p + i, n_plane))
        lists.append(remote(routes_hbm, rbuf2.at[p], rt2_send.at[i, 0], rt2_recv.at[i, 0], to))
        lists.append(remote(rw_hbm, wbuf2.at[p], rt2_send.at[i, 1], rt2_recv.at[i, 1], to))
    for copy in lists:
        copy.start()

    lane = lax.broadcasted_iota(jnp.int32, (block, block), 1)
    sub = lax.broadcasted_iota(jnp.int32, (block, block), 0)
    below = (sub < lane).astype(BF)

    def slots(chosen, weight, expert, put):
        count = expert.shape[0]
        named = jnp.zeros((count, block), F32)
        share = jnp.zeros((count, block), F32)
        for i in range(chosen.shape[0]):
            hit = jnp.broadcast_to(chosen[i:i + 1], (count, block)) == expert
            named = jnp.where(hit, 1.0, named)
            share = jnp.where(hit, jnp.broadcast_to(weight[i:i + 1], (count, block)), share)
        place = dot(named.astype(BF), below)
        place = jnp.where(named > 0.0, place, -1.0)
        seat = lax.broadcasted_iota(jnp.int32, (cap, block), 0).astype(F32)
        chosen_rows, pieces = [], []
        for j in range(count):
            here = jnp.broadcast_to(place[j:j + 1], (cap, block)) == seat
            chosen_rows.append(jnp.where(here, 1.0, 0.0).astype(BF))
            pieces.append(jnp.where(here, jnp.broadcast_to(share[j:j + 1], (cap, block)), 0.0))
        put(jnp.concatenate(chosen_rows, axis=0), jnp.concatenate(pieces, axis=0).T.astype(BF))

    def line_slots(k):
        b = ordered(k)
        group = lax.broadcasted_iota(jnp.int32, (peers, block), 0)

        def put(pick, share):
            select[k] = pick
            spread[k] = share

        slots(rbuf[b], wbuf[b], z * peers + lax.rem(rank + group, peers), put)

    def plane_slots(q):
        group = lax.broadcasted_iota(jnp.int32, (nz * n_core, block), 0)

        def put(pick, share):
            select2[q] = pick
            spread2[q] = share

        slots(rbuf2[q], wbuf2[q], group // n_core * peers + p * n_core + lax.rem(group, n_core), put)

    for load in tables:
        load.wait()
    line_slots(0)

    for load in front:
        load.wait()
    for copy in notes + swaps:
        copy.wait_recv()
    for h in range(n_core):
        for i, dst in enumerate((ci_f, gi_f)):
            here = dst.at[h, pl.ds(pl.multiple_of(core * far, HALO), HALO)]
            remote(here, here, h_send.at[0, i], h_recv.at[h, i], partner).wait_recv()

    own, before_docs, after_docs = docs[0], docs[1], docs[2]
    first_half = core == 0
    wide = (8, block)

    def row(x):
        return jnp.broadcast_to(x.astype(F32), wide)

    cur = row(jnp.where(first_half, own[0:1], own[1:2]))
    left = row(jnp.where(first_half, before_docs[1:2], own[0:1]))
    right = row(jnp.where(first_half, own[1:2], after_docs[0:1]))
    lanes = lax.broadcasted_iota(jnp.int32, wide, 1)
    before = jnp.where(lanes == 0, pltpu.roll(left, 1, 1), pltpu.roll(cur, 1, 1))
    after = jnp.where(lanes == block - 1, pltpu.roll(right, block - 1, 1), pltpu.roll(cur, block - 1, 1))
    position = (me * n_core + core) * block + lanes
    has_before = (cur == before) & (position > 0)
    has_after = (cur == after) & (position < n_seq * n_core * block - 1)
    both = jnp.where(lax.broadcasted_iota(jnp.int32, wide, 0) == 0,
                     jnp.where(has_before, 1.0, 0.0), jnp.where(has_after, 1.0, 0.0))
    marks = jnp.concatenate([both] * (block // 8), axis=0).T
    keep_before, keep_after = marks[:, 0:1], marks[:, 1:2]

    for h in range(n_core):
        prod[...] = gi_f[h].astype(F32) * ci_f[h].astype(F32)
        conv = (
            taps_f[h, 0:1, :] * (prod[HALO - 1:HALO - 1 + block, :] * keep_before)
            + taps_f[h, 1:2, :] * prod[HALO:HALO + block, :]
            + taps_f[h, 2:3, :] * (prod[HALO + 1:HALO + 1 + block, :] * keep_after)
        )
        mixed[:, h * half:(h + 1) * half] = (go_f[h].astype(F32) * conv).astype(BF)

    project.wait()
    square = jnp.zeros((block, 128), F32)
    for q in range(width // wide_col):
        cols = slice(q * wide_col, (q + 1) * wide_col)
        value = stream[:, cols].astype(F32) + dot(mixed[...], wp[:, cols])
        hidden[:, cols] = value
        value = value * value
        for i in range(wide_col // 128):
            square = square + value[:, i * 128:(i + 1) * 128]
    scale = lax.rsqrt(jnp.sum(square, axis=1, keepdims=True) / width + 1e-05)

    def chunk(q):
        return pl.ds(pl.multiple_of(q * col, col), col)

    def z_up(h, q):
        b = z - h
        piece = zbuf.at[b, :, chunk(q)]
        return remote(piece, piece, zu_send.at[h, q], z_recv.at[b, q], at_z(z + 1))

    def z_down(h, q):
        b = z + h
        piece = zbuf.at[b, :, chunk(q)]
        return remote(piece, piece, zd_send.at[h, q], z_recv.at[b, q], at_z(z - 1))

    def normed(cols):
        return (hidden[:, cols] * scale * gain[:, cols]).astype(BF)

    side = slice(main, width)
    pslab[p] = normed(side)
    s_copies = [
        remote(pslab.at[p], pslab.at[p], s_send.at[i], s_recv.at[p], in_plane(lax.rem(p + i, n_plane)))
        for i in range(1, n_plane)
    ]
    for copy in s_copies:
        copy.start()
    for q in range(nc):
        cols = slice(q * col, (q + 1) * col)
        zbuf[z, :, cols] = normed(cols)

    for q in range(nc):
        @pl.when(z < nz - 1)
        def _():
            z_up(0, q).start()

        @pl.when(z > 0)
        def _():
            z_down(0, q).start()

    def pump(h, q):
        @pl.when(z >= h)
        def _():
            piece = zbuf.at[z - h, :, chunk(q)]
            remote(piece, piece, zu_send.at[h, q], z_recv.at[z - h, q], at_z(z)).wait_recv()

            @pl.when(z < nz - 1)
            def _():
                z_up(h, q).start()

        @pl.when(z + h < nz)
        def _():
            piece = zbuf.at[z + h, :, chunk(q)]
            remote(piece, piece, zd_send.at[h, q], z_recv.at[z + h, q], at_z(z)).wait_recv()

            @pl.when(z > 0)
            def _():
                z_down(h, q).start()

    def seat_of(source):
        return pl.multiple_of((lax.rem(source, n_core) * n_plane + source // n_core) * cap, HALO)

    my_seat = seat_of(rank)

    def a_copy(k, j, q):
        b = ordered(k)
        return remote(
            outgoing.at[k, pl.ds((j - 1) * cap, cap), chunk(q)], arrived.at[b, pl.ds(my_seat, cap), chunk(q)],
            a_send.at[b, q], a_recv.at[b, q], plane_peer(j))

    def a_all(k, q):
        b = ordered(k)
        return remote(outgoing.at[k, :, chunk(q)], arrived.at[b, pl.ds(cap, rows - cap), chunk(q)],
                      a_send.at[b, q], a_recv.at[b, q], plane_peer(1))

    def r_copy(k, j, q):
        b = ordered(k)
        seat = seat_of(lax.rem(rank + peers - j, peers))
        return remote(
            arrived.at[b, pl.ds(seat, cap), chunk(q)], returned.at[b, pl.ds(j * cap, cap), chunk(q)],
            r_send.at[b, q], r_recv.at[b, q], plane_peer(peers - j))

    def r_all(k, q):
        b = ordered(k)
        return remote(
            arrived.at[b, pl.ds(cap, rows - cap), chunk(q)], returned.at[b, pl.ds(cap, rows - cap), chunk(q)],
            r_send.at[b, q], r_recv.at[b, q], plane_peer(1))

    def dispatch(k):
        b = ordered(k)

        @pl.loop(0, nc)
        def _(q):
            if k:
                pump(k, q)
            cols = chunk(q)
            picked = dot(select[k], zbuf[b, :, cols]).astype(BF)
            arrived[b, pl.ds(my_seat, cap), cols] = picked[:cap]
            outgoing[k, :, cols] = picked[cap:]
            for j in range(1, peers):
                a_copy(k, j, q).start()

    lot = n_plane * cap
    side_ref = pl.ds(main, slab)
    my_lot = pl.multiple_of(core * lot, HALO)
    other_lot = pl.multiple_of(other * lot, HALO)

    def v_copy(b, c):
        return remote(
            outgoing2.at[b, c], arrived.at[z, pl.ds(my_lot, lot), side_ref],
            v_send.at[b, c], v_recv.at[z, core], {"sp": b * n_plane + p, "tp": c})

    def v_wait(b, c):
        piece = arrived.at[b, pl.ds(pl.multiple_of(c * lot, HALO), lot), side_ref]
        remote(piece, piece, v_send.at[b, c], v_recv.at[b, c], partner).wait_recv()

    def side_pick():
        for q in range(n_plane):
            @pl.when(p != q)
            def _():
                remote(pslab.at[q], pslab.at[q], s_send.at[1], s_recv.at[q], partner).wait_recv()

            plane_slots(q)
            picked = dot(select2[q], pslab[q]).astype(BF)
            for b in range(nz):
                for c in range(n_core):
                    at = (b * n_core + c) * cap
                    outgoing2[b, c, q * cap:(q + 1) * cap, :] = picked[at:at + cap]
        arrived[z, pl.ds(my_lot, lot), side] = outgoing2[z, core]
        v_copy(z, other).start()

    def side_send(h):
        @pl.when(z + h < nz)
        def _():
            for c in range(n_core):
                v_copy(z + h, jnp.int32(c)).start()

        @pl.when(z >= h)
        def _():
            for c in range(n_core):
                v_copy(z - h, jnp.int32(c)).start()

    def w_copy(b, c):
        piece = arrived.at[b, pl.ds(pl.multiple_of(c * lot, HALO), lot), side_ref]
        return remote(piece, returned2.at[z, core], w_send.at[b, c], w_recv.at[z, core],
                      {"sp": b * n_plane + p, "tp": c})

    def f_copy(q):
        return remote(partial2.at[q], summed2.at[p], f_send.at[q], f_recv.at[p], in_plane(q))

    def side_combine():
        for b in range(nz):
            for c in range(n_core):
                @pl.when((z != b) | (core != c))
                def _():
                    piece = returned2.at[b, c]
                    remote(piece, piece, w_send.at[b, c], w_recv.at[b, c], partner).wait_recv()
        for q in range(n_plane):
            results = jnp.concatenate(
                [returned2[b, c, q * cap:(q + 1) * cap, :] for b in range(nz) for c in range(n_core)], axis=0)
            total = dot(spread2[q], results)

            @pl.when(p == q)
            def _():
                hidden[:, side] = hidden[:, side] + total

            @pl.when(p != q)
            def _():
                partial2[q] = total.astype(BF)
                f_copy(jnp.int32(q)).start()

    fcol = tile_of(ff, 256)

    def expert(k):
        b = ordered(k)
        if k == 0:
            for load in weights:
                load.wait()
            v_wait(z, other)
        else:
            for c in range(n_core):
                v_wait(b, c)

        @pl.loop(0, nc)
        def _(q):
            a_all(k, q).wait_recv()

        @pl.loop(0, ff // fcol)
        def _(i):
            cols = pl.ds(pl.multiple_of(i * fcol, fcol), fcol)
            gate = jnp.minimum(dot(arrived[b], wg[:, cols]), 7.0)
            upper = jnp.clip(dot(arrived[b], wu[:, cols]), -7.0, 7.0)
            act[:, cols] = ((upper + 1.0) * gate * jax.nn.sigmoid(1.702 * gate)).astype(BF)

        arrived[b, :, side] = dot(act[...], wd[:, side]).astype(BF)
        if k == 0:
            returned2[z, core] = arrived[z, pl.ds(my_lot, lot), side]
            w_copy(z, other).start()
        else:
            for c in range(n_core):
                w_copy(b, c).start()

        @pl.loop(0, nc)
        def _(q):
            cols = chunk(q)
            arrived[b, :, cols] = dot(act[...], wd[:, cols]).astype(BF)
            returned[b, 0:cap, cols] = arrived[b, pl.ds(my_seat, cap), cols]
            if k == nz - 1:
                give(k, q)

    def give(k, q):
        for j in range(1, peers):
            r_copy(k, j, q).start()

    def chained(b):
        return ((b < z) & (z < nz - 1)) | ((b > z) & (z > 0))

    def p_copy(k, q):
        b = ordered(k)
        down = b < z
        seat = jnp.where(down & (b == z - 1), nz, b)
        return remote(partial.at[k - 1, :, chunk(q)], chain.at[seat, :, chunk(q)],
                      p_send.at[k, q], p_recv.at[seat, q], at_z(jnp.where(down, z - 1, z + 1)))

    def p_wait(seat, q):
        piece = chain.at[seat, :, chunk(q)]
        remote(piece, piece, p_send.at[0, q], p_recv.at[seat, q], at_z(z)).wait_recv()

    def combine(k):
        b = ordered(k)

        @pl.loop(0, nc)
        def _(q):
            cols = chunk(q)
            r_all(k, q).wait_recv()
            total = dot(spread[k], returned[b, :, cols])
            if k == 0:
                hidden[:, cols] = hidden[:, cols] + total
            else:
                @pl.when(chained(b))
                def _():
                    p_wait(b, q)
                    partial[k - 1, :, cols] = (total + chain[b, :, cols].astype(F32)).astype(BF)

                @pl.when(jnp.logical_not(chained(b)))
                def _():
                    partial[k - 1, :, cols] = total.astype(BF)

                p_copy(k, q).start()

    dispatch(0)
    for copy in lists:
        copy.wait_recv()
    side_pick()
    for k in range(1, nz):
        line_slots(k)
        dispatch(k)
        side_send(k)
        if k < nz - 1:
            expert(k - 1)

    def give_all(k, low, high):
        @pl.loop(low, high)
        def _(q):
            give(k, q)

    give_all(0, 0, nc // 2)
    expert(nz - 2)
    expert(nz - 1)
    for k in range(nz - 2, 0, -1):
        give_all(k, 0, nc)
    combine(nz - 1)
    side_combine()
    give_all(0, nc // 2, nc)
    for k in range(nz - 2, -1, -1):
        combine(k)
    for q in range(n_plane):
        @pl.when(p != q)
        def _():
            remote(summed2.at[q], summed2.at[q], f_send.at[q], f_recv.at[q], partner).wait_recv()
            hidden[:, side] = hidden[:, side] + summed2[q].astype(F32)
    out_ref[:, side] = hidden[:, side].astype(BF)

    @pl.loop(0, nc)
    def _(q):
        cols = chunk(q)

        @pl.when(z > 0)
        def _():
            p_wait(z, q)
            hidden[:, cols] = hidden[:, cols] + chain[z, :, cols].astype(F32)

        @pl.when(z < nz - 1)
        def _():
            p_wait(nz, q)
            hidden[:, cols] = hidden[:, cols] + chain[nz, :, cols].astype(F32)

        out_ref[:, cols] = hidden[:, cols].astype(BF)

    for copy in halos + notes + swaps + lists + s_copies:
        copy.wait_send()
    for b in range(nz):
        for c in range(n_core):
            @pl.when((z != b) | (core != c))
            def _():
                v_copy(jnp.int32(b), jnp.int32(c)).wait_send()
                w_copy(jnp.int32(b), jnp.int32(c)).wait_send()
    for q in range(n_plane):
        @pl.when(p != q)
        def _():
            f_copy(jnp.int32(q)).wait_send()

    @pl.loop(0, nc)
    def _(q):
        for h in range(nz):
            @pl.when((z >= h) & (z < nz - 1))
            def _():
                z_up(h, q).wait_send()

            @pl.when((z + h < nz) & (z > 0))
            def _():
                z_down(h, q).wait_send()
        for k in range(nz):
            a_all(k, q).wait_send()
            r_all(k, q).wait_send()
            if k:
                p_copy(k, q).wait_send()


def layer(n_seq, nz, n_plane, n_core, cap, *args):
    tok, half = args[0].shape
    block, width = args[6].shape
    ff = args[10].shape[1]
    peers = n_plane * n_core
    rows = peers * cap
    topk = args[8].shape[0]
    channels = half * n_core
    frame = block + 2 * HALO
    slab = SLAB if width > 2 * SLAB else 128
    main = width - slab
    col = tile_of(main, COL)
    nc = main // col
    lot = n_plane * cap
    hbm = pl.BlockSpec(memory_space=pl.ANY)
    vmem = pl.BlockSpec(memory_space=pltpu.VMEM)
    dma = pltpu.SemaphoreType.DMA
    return pl.pallas_call(
        functools.partial(layer_kernel, n_seq, nz, n_plane, n_core, cap, col, slab),
        out_shape=jax.ShapeDtypeStruct((block, width), BF),
        in_specs=[hbm] * len(args),
        out_specs=vmem,
        scratch_shapes=[
            pltpu.VMEM((width, ff), BF),
            pltpu.VMEM((width, ff), BF),
            pltpu.VMEM((ff, width), BF),
            pltpu.VMEM((channels, width), BF),
            pltpu.VMEM((n_core, frame, half), BF),
            pltpu.VMEM((n_core, frame, half), BF),
            pltpu.VMEM((n_core, block, half), BF),
            pltpu.VMEM((n_core,) + args[3].shape, F32),
            pltpu.VMEM((3, n_core, block), jnp.int32),
            pltpu.VMEM((frame, half), F32),
            pltpu.VMEM((block, channels), BF),
            pltpu.VMEM((block, width), BF),
            pltpu.VMEM((1, width), F32),
            pltpu.VMEM((block, width), F32),
            pltpu.VMEM((nz, topk, block), jnp.int32),
            pltpu.VMEM((nz, topk, block), F32),
            pltpu.VMEM((nz, rows, block), BF),
            pltpu.VMEM((nz, block, rows), BF),
            pltpu.VMEM((nz, block, main), BF),
            pltpu.VMEM((nz, rows - cap, main), BF),
            pltpu.VMEM((nz, rows, width), BF),
            pltpu.VMEM((rows, ff), BF),
            pltpu.VMEM((nz, rows, main), BF),
            pltpu.VMEM((nz - 1, block, main), BF),
            pltpu.VMEM((nz + 1, block, main), BF),
            pltpu.VMEM((n_plane, topk, block), jnp.int32),
            pltpu.VMEM((n_plane, topk, block), F32),
            pltpu.VMEM((n_plane, nz * n_core * cap, block), BF),
            pltpu.VMEM((n_plane, block, nz * n_core * cap), BF),
            pltpu.VMEM((n_plane, block, slab), BF),
            pltpu.VMEM((nz, n_core, lot, slab), BF),
            pltpu.VMEM((nz, n_core, lot, slab), BF),
            pltpu.VMEM((n_plane, block, slab), BF),
            pltpu.VMEM((n_plane, block, slab), BF),
            dma((15,)), dma((4,)), dma((4,)), dma((2, 2)), dma((n_core, 2)),
            dma((2,)), dma((2,)), dma((nz, 2)), dma((nz, 2)),
            dma((nz, nc)), dma((nz, nc)), dma((nz, nc)),
            dma((nz, nc)), dma((nz, nc)), dma((nz, nc)), dma((nz, nc)),
            dma((nz, nc)), dma((nz + 1, nc)),
            dma((n_plane, 2)), dma((n_plane, 2)), dma((n_plane,)), dma((n_plane,)),
            dma((nz, n_core)), dma((nz, n_core)), dma((nz, n_core)), dma((nz, n_core)),
            dma((n_plane,)), dma((n_plane,)),
        ],
        compiler_params=pltpu.CompilerParams(
            collective_id=0, has_side_effects=True, vmem_limit_bytes=62 * 2**20),
        name="mixer_experts",
    )(*args)


def per_device(
    conv_in, gate_outer, gate_inner, tap_weights, doc_ids, w_proj, stream, norm_gain,
    routes, route_weights, w_gate, w_up, w_down,
):
    n_seq = lax.axis_size("sp")
    n_core = lax.axis_size("tp")
    tok_dev = conv_in.shape[0]
    topk = routes.shape[1]
    capacity = max(2, 2 * tok_dev * topk // (n_core * n_seq * n_core))
    capacity = -(-capacity // 16) * 16
    nz = max(d for d in range(1, math.isqrt(n_seq) + 1) if n_seq % d == 0)
    return layer(
        n_seq, nz, n_seq // nz, n_core, capacity,
        conv_in, gate_outer, gate_inner, tap_weights,
        doc_ids.reshape(n_core, tok_dev // n_core), w_proj, stream, norm_gain.reshape(1, -1),
        routes.T, route_weights.T, w_gate[0], w_up[0], w_down[0])


def solution(mesh):
    in_specs = (
        P("sp", "tp"),
        P("sp", "tp"),
        P("sp", "tp"),
        P(None, "tp"),
        P("sp"),
        P(),
        P(("sp", "tp"), None),
        P(),
        P(("sp", "tp"), None),
        P(("sp", "tp"), None),
        P(("sp", "tp"), None, None),
        P(("sp", "tp"), None, None),
        P(("sp", "tp"), None, None),
    )
    return jax.shard_map(
        per_device, mesh=mesh, in_specs=in_specs, out_specs=P(("sp", "tp"), None), check_vma=False
    )
```

```python
import functools
import math

import jax
import jax.numpy as jnp
from jax import lax
from jax.experimental import pallas as pl
from jax.experimental.pallas import tpu as pltpu
from jax.sharding import PartitionSpec as P

MESH = pl.DeviceIdType.MESH
HALO = 16
SLAB = 384
CHUNKS = 2
BF = jnp.bfloat16
F32 = jnp.float32


def dot(a, b):
    return jnp.dot(a, b, preferred_element_type=F32)


def tile_of(size, most):
    return next(t for t in range(most, 0, -128) if size % t == 0)


def nearest_first(nz):
    return [sorted(range(nz), key=lambda b: (abs(b - z), abs(2 * b - nz + 1) * (1 if nz > 2 else 0), b))
            for z in range(nz)]


def layer_kernel(
    n_seq, nz, n_plane, n_core, cap, cuts, slab,
    ci_hbm, go_hbm, gi_hbm, taps_hbm, docs_hbm, wp_hbm, stream_hbm, gain_hbm,
    routes_hbm, rw_hbm, wg_hbm, wu_hbm, wd_hbm,
    out_ref,
    wg, wu, wd, wp, raw, frames, go_f, taps_f, docs, prod, mixed, stream, gain, hidden,
    rbuf, wbuf, select, spread, zbuf, outgoing, arrived, act, returned, partial, chain,
    rbuf2, wbuf2, select2, spread2, pslab, outgoing2, returned2, partial2, summed2,
    l_sem, e_send, e_recv, h_send, h_recv, d_send, d_recv, rt_send, rt_recv,
    z_send, z_recv, a_send, a_recv, r_send, r_recv, p_send, p_recv,
    s_send, s_recv, v_send, v_recv, w_send, w_recv, f_send, f_recv,
):
    peers = n_plane * n_core
    rows = peers * cap
    block, width = hidden.shape
    ff = wg.shape[1]
    half = ci_hbm.shape[1]
    span = block + HALO
    main = width - slab
    nc = len(cuts)
    wide_col = tile_of(width, 512)
    me = lax.axis_index("sp")
    core = lax.axis_index("tp")
    z, p = me // n_plane, lax.rem(me, n_plane)
    rank = p * n_core + core
    other = 1 - core

    def at_z(b):
        return {"sp": b * n_plane + p, "tp": core}

    def in_plane(q):
        return {"sp": z * n_plane + q, "tp": core}

    def plane_peer(j):
        q = lax.rem(rank + j, peers)
        return {"sp": z * n_plane + q // n_core, "tp": lax.rem(q, n_core)}

    nxt, prv = me + 1, me - 1
    order = nearest_first(nz)

    def ordered(k):
        total = jnp.int32(0)
        for i in range(nz):
            total = total + jnp.where(z == i, order[i][k], 0)
        return total

    def remote(src, dst, send, recv, to):
        return pltpu.make_async_remote_copy(
            src_ref=src, dst_ref=dst, send_sem=send, recv_sem=recv,
            device_id=to, device_id_type=MESH)

    mine = pl.multiple_of(core * (block - HALO), HALO)
    theirs = pl.multiple_of(other * (block - HALO), HALO)
    my_at = pl.multiple_of(other * HALO, HALO)
    their_at = pl.multiple_of(core * HALO, HALO)

    def local(i, src, dst):
        return pltpu.make_async_copy(src, dst, l_sem.at[i])

    hbm_in = (ci_hbm, gi_hbm)
    front = [
        local(0, src.at[pl.ds(mine, span)], frames.at[i, core, pl.ds(my_at, span)]) for i, src in enumerate(hbm_in)
    ] + [
        local(1, go_hbm.at[pl.ds(pl.multiple_of(core * block, HALO), block)], go_f.at[core]),
        local(2, taps_hbm, taps_f.at[core]),
        local(3, stream_hbm, stream),
        local(4, gain_hbm, gain),
    ]
    own_frames = frames.at[:, core, pl.ds(my_at, span)]
    front_waits = [pltpu.make_async_copy(own_frames, own_frames, l_sem.at[0])] + front[2:]
    papers = local(5, docs_hbm, docs.at[0])
    stage = [local(6, src, raw.at[i]) for i, src in enumerate((ci_hbm, gi_hbm, go_hbm))]
    stage_wait = pltpu.make_async_copy(raw, raw, l_sem.at[6])
    tables = [local(7, routes_hbm, rbuf.at[z]), local(7, rw_hbm, wbuf.at[z]),
              local(7, routes_hbm, rbuf2.at[p]), local(7, rw_hbm, wbuf2.at[p])]
    topk = routes_hbm.shape[0]

    def lists_of(count):
        return hidden.at[pl.ds(0, 2 * topk), pl.ds(0, count * block)]

    tables_wait = pltpu.make_async_copy(lists_of(2), lists_of(2), l_sem.at[7])
    project = local(8, wp_hbm, wp)
    weights = [local(9, wg_hbm, wg), local(10, wu_hbm, wu), local(11, wd_hbm, wd)]
    for load in stage + [papers] + front + tables:
        load.start()

    barrier = pltpu.get_barrier_semaphore()

    def greet(to):
        pl.semaphore_signal(barrier, inc=1, device_id=to, device_id_type=MESH)

    for k in range(1, nz):
        greet(at_z(lax.rem(z + k, nz)))
        greet({"sp": lax.rem(z + k, nz) * n_plane + p, "tp": other})
    for j in range(1, peers):
        greet(plane_peer(j))
    has_prv, has_nxt = me > 0, me < n_seq - 1
    for n, there in ((nxt, has_nxt), (prv, has_prv)):
        @pl.when(there)
        def _():
            for c in range(n_core):
                greet({"sp": n, "tp": jnp.int32(c)})
    sides = jnp.where(has_prv, n_core, 0) + jnp.where(has_nxt, n_core, 0)
    pl.semaphore_wait(barrier, 2 * (nz - 1) + peers - 1 + sides)

    edge = ci_hbm.shape[0] - HALO
    far = block + HALO
    partner = {"tp": other}
    to_next = [
        remote(raw.at[i, pl.ds(edge, HALO)], frames.at[i, core, pl.ds(0, HALO)],
               h_send.at[0], h_recv.at[0], {"sp": nxt, "tp": jnp.int32(0)}) for i in range(2)]
    to_prev = [
        remote(raw.at[i, pl.ds(0, HALO)], frames.at[i, core, pl.ds(far, HALO)],
               h_send.at[1], h_recv.at[0], {"sp": prv, "tp": jnp.int32(1)}) for i in range(2)]
    halo_part = frames.at[:, core, pl.ds(0, HALO)]
    docs_next = remote(docs.at[0], docs.at[1], d_send.at[0], d_recv.at[0], {"sp": nxt, "tp": core})
    docs_prev = remote(docs.at[0], docs.at[2], d_send.at[0], d_recv.at[0], {"sp": prv, "tp": core})
    first_half = core == 0
    inside = (first_half & has_prv) | (jnp.logical_not(first_half) & has_nxt)
    swaps = [
        remote(raw.at[i, pl.ds(theirs, span)], frames.at[i, core, pl.ds(their_at, span)],
               e_send.at[0], e_recv.at[0], partner) for i in range(2)
    ] + [
        remote(raw.at[2, pl.ds(pl.multiple_of(other * block, HALO), block)], go_f.at[core],
               e_send.at[1], e_recv.at[1], partner),
        remote(taps_hbm, taps_f.at[core], e_send.at[2], e_recv.at[2], partner),
    ]
    their_frames = frames.at[:, core, pl.ds(their_at, span)]
    swap_waits = [remote(their_frames, their_frames, e_send.at[0], e_recv.at[0], partner)] + swaps[2:]
    stage_wait.wait()
    papers.wait()
    for copies, there in ((to_next, has_nxt), (to_prev, has_prv)):
        @pl.when(there)
        def _():
            for copy in copies:
                copy.start()

    @pl.when(first_half & has_nxt)
    def _():
        docs_next.start()

    @pl.when(jnp.logical_not(first_half) & has_prv)
    def _():
        docs_prev.start()

    for copy in swaps:
        copy.start()
    project.start()
    lists = []
    for k in range(1, nz):
        to = at_z(lax.rem(z + k, nz))
        lists.append(remote(routes_hbm, rbuf.at[z], rt_send.at[0], rt_recv.at[0], to))
        lists.append(remote(rw_hbm, wbuf.at[z], rt_send.at[0], rt_recv.at[0], to))
    for i in range(1, n_plane):
        to = in_plane(lax.rem(p + i, n_plane))
        lists.append(remote(routes_hbm, rbuf2.at[p], rt_send.at[1], rt_recv.at[1], to))
        lists.append(remote(rw_hbm, wbuf2.at[p], rt_send.at[1], rt_recv.at[1], to))
    for copy in lists:
        copy.start()
    list_waits = [
        remote(lists_of(n - 1), lists_of(n - 1), rt_send.at[i], rt_recv.at[i], partner)
        for i, n in enumerate((nz, n_plane))
    ]

    lane = lax.broadcasted_iota(jnp.int32, (block, block), 1)
    sub = lax.broadcasted_iota(jnp.int32, (block, block), 0)
    below = (sub < lane).astype(BF)

    def slots(chosen, weight, expert, put):
        count = expert.shape[0]
        named = jnp.zeros((count, block), F32)
        share = jnp.zeros((count, block), F32)
        for i in range(chosen.shape[0]):
            hit = jnp.broadcast_to(chosen[i:i + 1], (count, block)) == expert
            named = jnp.where(hit, 1.0, named)
            share = jnp.where(hit, jnp.broadcast_to(weight[i:i + 1], (count, block)), share)
        place = dot(named.astype(BF), below)
        place = jnp.where(named > 0.0, place, -1.0)
        seat = lax.broadcasted_iota(jnp.int32, (cap, block), 0).astype(F32)
        chosen_rows, pieces = [], []
        for j in range(count):
            here = jnp.broadcast_to(place[j:j + 1], (cap, block)) == seat
            chosen_rows.append(jnp.where(here, 1.0, 0.0).astype(BF))
            pieces.append(jnp.where(here, jnp.broadcast_to(share[j:j + 1], (cap, block)), 0.0))
        put(jnp.concatenate(chosen_rows, axis=0), jnp.concatenate(pieces, axis=0).T.astype(BF))

    def line_slots(k):
        b = ordered(k)
        group = lax.broadcasted_iota(jnp.int32, (peers, block), 0)

        def put(pick, share):
            select[k] = pick
            spread[k] = share

        slots(rbuf[b], wbuf[b], z * peers + lax.rem(rank + group, peers), put)

    def plane_slots(q):
        group = lax.broadcasted_iota(jnp.int32, (nz * n_core, block), 0)

        def put(pick, share):
            select2[q] = pick
            spread2[q] = share

        slots(rbuf2[q], wbuf2[q], group // n_core * peers + p * n_core + lax.rem(group, n_core), put)

    tables_wait.wait()
    line_slots(0)

    for load in front_waits:
        load.wait()
    for copy in swap_waits:
        copy.wait_recv()

    halo_at = pl.ds(pl.multiple_of(core * far, HALO), HALO)

    @pl.when(inside)
    def _():
        docs_next.wait_recv()
        here = frames.at[:, :, halo_at]
        remote(here, here, h_send.at[0], h_recv.at[0], partner).wait_recv()

    @pl.when(jnp.logical_not(inside))
    def _():
        for h in range(n_core):
            for i in range(2):
                frames[i, h, halo_at, :] = jnp.zeros((HALO, half), BF)

    @pl.when(jnp.logical_not(first_half & has_prv))
    def _():
        docs[1] = docs[0]

    @pl.when(first_half | jnp.logical_not(has_nxt))
    def _():
        docs[2] = docs[0]

    for load in weights:
        load.start()

    own, before_docs, after_docs = docs[0], docs[1], docs[2]
    wide = (8, block)

    def row(x):
        return jnp.broadcast_to(x.astype(F32), wide)

    cur = row(jnp.where(first_half, own[0:1], own[1:2]))
    left = row(jnp.where(first_half, before_docs[1:2], own[0:1]))
    right = row(jnp.where(first_half, own[1:2], after_docs[0:1]))
    lanes = lax.broadcasted_iota(jnp.int32, wide, 1)
    before = jnp.where(lanes == 0, pltpu.roll(left, 1, 1), pltpu.roll(cur, 1, 1))
    after = jnp.where(lanes == block - 1, pltpu.roll(right, block - 1, 1), pltpu.roll(cur, block - 1, 1))
    position = (me * n_core + core) * block + lanes
    has_before = (cur == before) & (position > 0)
    has_after = (cur == after) & (position < n_seq * n_core * block - 1)
    both = jnp.where(lax.broadcasted_iota(jnp.int32, wide, 0) == 0,
                     jnp.where(has_before, 1.0, 0.0), jnp.where(has_after, 1.0, 0.0))
    marks = jnp.concatenate([both] * (block // 8), axis=0).T
    keep_before, keep_after = marks[:, 0:1], marks[:, 1:2]

    for h in range(n_core):
        prod[...] = frames[1, h].astype(F32) * frames[0, h].astype(F32)
        conv = (
            taps_f[h, 0:1, :] * (prod[HALO - 1:HALO - 1 + block, :] * keep_before)
            + taps_f[h, 1:2, :] * prod[HALO:HALO + block, :]
            + taps_f[h, 2:3, :] * (prod[HALO + 1:HALO + 1 + block, :] * keep_after)
        )
        mixed[:, h * half:(h + 1) * half] = (go_f[h].astype(F32) * conv).astype(BF)

    project.wait()
    square = jnp.zeros((block, 128), F32)
    for q in range(width // wide_col):
        cols = slice(q * wide_col, (q + 1) * wide_col)
        value = stream[:, cols].astype(F32) + dot(mixed[...], wp[:, cols])
        hidden[:, cols] = value
        value = value * value
        for i in range(wide_col // 128):
            square = square + value[:, i * 128:(i + 1) * 128]
    scale = lax.rsqrt(jnp.sum(square, axis=1, keepdims=True) / width + 1e-05)

    def chunk(q):
        return pl.ds(*cuts[q])

    def z_up(h, q):
        b = z - h
        piece = zbuf.at[b, :, chunk(q)]
        return remote(piece, piece, z_send.at[0], z_recv.at[b, q], at_z(z + 1))

    def z_down(h, q):
        b = z + h
        piece = zbuf.at[b, :, chunk(q)]
        return remote(piece, piece, z_send.at[0], z_recv.at[b, q], at_z(z - 1))

    def normed(cols):
        return (hidden[:, cols] * scale * gain[:, cols]).astype(BF)

    side = slice(main, width)
    pslab[p] = normed(side)
    s_copies = [
        remote(pslab.at[p], pslab.at[p], s_send.at[0], s_recv.at[0], in_plane(lax.rem(p + i, n_plane)))
        for i in range(1, n_plane)
    ]
    for copy in s_copies:
        copy.start()
    for q in range(nc):
        zbuf[z, :, chunk(q)] = normed(chunk(q))

    for q in range(nc):
        @pl.when(z < nz - 1)
        def _():
            z_up(0, q).start()

        @pl.when(z > 0)
        def _():
            z_down(0, q).start()

    def pump(h, q):
        @pl.when(z >= h)
        def _():
            piece = zbuf.at[z - h, :, chunk(q)]
            remote(piece, piece, z_send.at[0], z_recv.at[z - h, q], at_z(z)).wait_recv()

            @pl.when(z < nz - 1)
            def _():
                z_up(h, q).start()

        @pl.when(z + h < nz)
        def _():
            piece = zbuf.at[z + h, :, chunk(q)]
            remote(piece, piece, z_send.at[0], z_recv.at[z + h, q], at_z(z)).wait_recv()

            @pl.when(z > 0)
            def _():
                z_down(h, q).start()

    def seat_of(source):
        return pl.multiple_of((lax.rem(source, n_core) * n_plane + source // n_core) * cap, HALO)

    my_seat = seat_of(rank)

    def a_copy(k, j, q):
        b = ordered(k)
        return remote(
            outgoing.at[k, pl.ds((j - 1) * cap, cap), chunk(q)], arrived.at[b, pl.ds(my_seat, cap), chunk(q)],
            a_send.at[0], a_recv.at[b], plane_peer(j))

    def a_all(k):
        b = ordered(k)
        return remote(outgoing.at[k], arrived.at[b, pl.ds(cap, rows - cap), pl.ds(0, main)],
                      a_send.at[0], a_recv.at[b], plane_peer(1))

    def r_copy(k, j, q):
        b = ordered(k)
        seat = seat_of(lax.rem(rank + peers - j, peers))
        return remote(
            arrived.at[b, pl.ds(seat, cap), chunk(q)], returned.at[b, pl.ds(j * cap, cap), chunk(q)],
            r_send.at[0], r_recv.at[b, q], plane_peer(peers - j))

    def r_all(k, q):
        b = ordered(k)
        return remote(
            arrived.at[b, pl.ds(cap, rows - cap), chunk(q)], returned.at[b, pl.ds(cap, rows - cap), chunk(q)],
            r_send.at[0], r_recv.at[b, q], plane_peer(1))

    def dispatch(k):
        b = ordered(k)

        for q in range(nc):
            if k:
                pump(k, q)
            cols = chunk(q)
            picked = dot(select[k], zbuf[b, :, cols]).astype(BF)
            arrived[b, pl.ds(my_seat, cap), cols] = picked[:cap]
            outgoing[k, :, cols] = picked[cap:]
            for j in range(1, peers):
                a_copy(k, j, q).start()

    lot = n_plane * cap
    side_ref = pl.ds(main, slab)
    my_lot = pl.multiple_of(core * lot, HALO)
    other_lot = pl.multiple_of(other * lot, HALO)

    def v_copy(b, c):
        return remote(
            outgoing2.at[b * n_core + c], arrived.at[z, pl.ds(my_lot, lot), side_ref],
            v_send.at[0], v_recv.at[z], {"sp": b * n_plane + p, "tp": c})

    def v_wait(b, count):
        piece = arrived.at[b, pl.ds(0, count * lot), side_ref]
        remote(piece, piece, v_send.at[0], v_recv.at[b], partner).wait_recv()

    def rest(ref):
        return ref.at[pl.ds(0, ref.shape[0] - 1)]

    def all_of(ref, send, recv):
        return remote(ref, ref, send, recv, partner)

    s_all = all_of(rest(pslab), s_send.at[0], s_recv.at[0])
    v_all = all_of(rest(outgoing2), v_send.at[0], v_recv.at[0])
    w_all = all_of(rest(returned2), w_send.at[0], w_recv.at[0])
    f_all = all_of(rest(partial2), f_send.at[0], f_recv.at[0])

    def side_pick():
        s_all.wait_recv()
        for q in range(n_plane):
            plane_slots(q)
            picked = dot(select2[q], pslab[q]).astype(BF)
            for b in range(nz):
                for c in range(n_core):
                    at = (b * n_core + c) * cap
                    outgoing2[b * n_core + c, q * cap:(q + 1) * cap, :] = picked[at:at + cap]
        arrived[z, pl.ds(my_lot, lot), side] = outgoing2[z * n_core + core]
        v_copy(z, other).start()

    def side_send(h):
        @pl.when(z + h < nz)
        def _():
            for c in range(n_core):
                v_copy(z + h, jnp.int32(c)).start()

        @pl.when(z >= h)
        def _():
            for c in range(n_core):
                v_copy(z - h, jnp.int32(c)).start()

    def w_copy(b, c):
        piece = arrived.at[b, pl.ds(pl.multiple_of(c * lot, HALO), lot), side_ref]
        return remote(piece, returned2.at[z * n_core + core], w_send.at[0], w_recv.at[0],
                      {"sp": b * n_plane + p, "tp": c})

    def f_copy(q):
        return remote(partial2.at[q], summed2.at[p], f_send.at[0], f_recv.at[0], in_plane(q))

    def side_combine():
        w_all.wait_recv()
        for q in range(n_plane):
            results = jnp.concatenate(
                [returned2[b, q * cap:(q + 1) * cap, :] for b in range(nz * n_core)], axis=0)
            total = dot(spread2[q], results)

            @pl.when(p == q)
            def _():
                hidden[:, side] = hidden[:, side] + total

            @pl.when(p != q)
            def _():
                partial2[q] = total.astype(BF)
                f_copy(jnp.int32(q)).start()

    fcol = tile_of(ff, 256)

    def expert(k):
        b = ordered(k)
        if k == 0:
            for load in weights:
                load.wait()
            v_wait(z, n_core - 1)
        else:
            v_wait(b, n_core)

        a_all(k).wait_recv()

        @pl.loop(0, ff // fcol)
        def _(i):
            cols = pl.ds(pl.multiple_of(i * fcol, fcol), fcol)
            gate = jnp.minimum(dot(arrived[b], wg[:, cols]), 7.0)
            upper = jnp.clip(dot(arrived[b], wu[:, cols]), -7.0, 7.0)
            act[:, cols] = ((upper + 1.0) * gate * jax.nn.sigmoid(1.702 * gate)).astype(BF)

        arrived[b, :, side] = dot(act[...], wd[:, side]).astype(BF)
        if k == 0:
            returned2[z * n_core + core] = arrived[z, pl.ds(my_lot, lot), side]
            w_copy(z, other).start()
        else:
            for c in range(n_core):
                w_copy(b, c).start()

        for q in range(nc):
            cols = chunk(q)
            arrived[b, :, cols] = dot(act[...], wd[:, cols]).astype(BF)
            returned[b, 0:cap, cols] = arrived[b, pl.ds(my_seat, cap), cols]
            if k == nz - 1:
                give(k, q)

    def give(k, q):
        for j in range(1, peers):
            r_copy(k, j, q).start()

    def chained(b):
        return ((b < z) & (z < nz - 1)) | ((b > z) & (z > 0))

    def p_copy(k, q):
        b = ordered(k)
        down = b < z
        seat = jnp.where(down & (b == z - 1), nz, b)
        return remote(partial.at[k - 1, :, chunk(q)], chain.at[seat, :, chunk(q)],
                      p_send.at[0], p_recv.at[seat, q], at_z(jnp.where(down, z - 1, z + 1)))

    def p_wait(seat, q):
        piece = chain.at[seat, :, chunk(q)]
        remote(piece, piece, p_send.at[0], p_recv.at[seat, q], at_z(z)).wait_recv()

    def combine(k):
        b = ordered(k)

        for q in range(nc):
            cols = chunk(q)
            r_all(k, q).wait_recv()
            total = dot(spread[k], returned[b, :, cols])
            if k == 0:
                hidden[:, cols] = hidden[:, cols] + total
            else:
                @pl.when(chained(b))
                def _():
                    p_wait(b, q)
                    partial[k - 1, :, cols] = (total + chain[b, :, cols].astype(F32)).astype(BF)

                @pl.when(jnp.logical_not(chained(b)))
                def _():
                    partial[k - 1, :, cols] = total.astype(BF)

                p_copy(k, q).start()

    def give_all(k, low, high):
        for q in range(low, high):
            give(k, q)

    dispatch(0)
    for copy in list_waits:
        copy.wait_recv()
    side_pick()
    for k in range(1, nz):
        line_slots(k)
        dispatch(k)
        side_send(k)
        if k < nz - 1:
            expert(k - 1)
    give_all(0, 0, nc)
    expert(nz - 2)
    expert(nz - 1)
    for k in range(nz - 2, 0, -1):
        give_all(k, 0, nc)
    combine(nz - 1)
    side_combine()
    for k in range(nz - 2, -1, -1):
        combine(k)
    f_all.wait_recv()
    for q in range(n_plane):
        @pl.when(p != q)
        def _():
            hidden[:, side] = hidden[:, side] + summed2[q].astype(F32)
    out_ref[:, side] = hidden[:, side].astype(BF)

    for q in range(nc):
        cols = chunk(q)

        @pl.when(z > 0)
        def _():
            p_wait(z, q)
            hidden[:, cols] = hidden[:, cols] + chain[z, :, cols].astype(F32)

        @pl.when(z < nz - 1)
        def _():
            p_wait(nz, q)
            hidden[:, cols] = hidden[:, cols] + chain[nz, :, cols].astype(F32)

        out_ref[:, cols] = hidden[:, cols].astype(BF)

    for i, there in enumerate((has_nxt, has_prv)):
        @pl.when(there)
        def _():
            remote(halo_part, halo_part, h_send.at[i], h_recv.at[0], partner).wait_send()

    @pl.when((first_half & has_nxt) | (jnp.logical_not(first_half) & has_prv))
    def _():
        docs_next.wait_send()

    for copy in swap_waits + list_waits + [s_all, v_all, w_all, f_all]:
        copy.wait_send()
    middle = (z > 0) & (z < nz - 1)

    @pl.when(middle)
    def _():
        remote(chain, chain, z_send.at[0], z_recv.at[0, 0], partner).wait_send()

    @pl.when(jnp.logical_not(middle))
    def _():
        remote(chain.at[0], chain.at[0], z_send.at[0], z_recv.at[0, 0], partner).wait_send()

    remote(outgoing, outgoing, a_send.at[0], a_recv.at[0], partner).wait_send()
    remote(outgoing, outgoing, r_send.at[0], r_recv.at[0, 0], partner).wait_send()
    remote(partial, partial, p_send.at[0], p_recv.at[0, 0], partner).wait_send()


def layer(n_seq, nz, n_plane, n_core, cap, *args):
    tok, half = args[0].shape
    block, width = args[6].shape
    ff = args[10].shape[1]
    peers = n_plane * n_core
    rows = peers * cap
    topk = args[8].shape[0]
    channels = half * n_core
    frame = block + 2 * HALO
    slab = SLAB if width > 2 * SLAB else 128
    main = width - slab
    parts = main // 128
    nc = min(CHUNKS, parts)
    edges = [-(-parts * i // nc) * 128 for i in range(nc + 1)]
    cuts = [(a, b - a) for a, b in zip(edges, edges[1:])]
    lot = n_plane * cap
    hbm = pl.BlockSpec(memory_space=pl.ANY)
    vmem = pl.BlockSpec(memory_space=pltpu.VMEM)
    dma = pltpu.SemaphoreType.DMA
    return pl.pallas_call(
        functools.partial(layer_kernel, n_seq, nz, n_plane, n_core, cap, cuts, slab),
        out_shape=jax.ShapeDtypeStruct((block, width), BF),
        in_specs=[hbm] * len(args),
        out_specs=vmem,
        scratch_shapes=[
            pltpu.VMEM((width, ff), BF),
            pltpu.VMEM((width, ff), BF),
            pltpu.VMEM((ff, width), BF),
            pltpu.VMEM((channels, width), BF),
            pltpu.VMEM((3, tok, half), BF),
            pltpu.VMEM((2, n_core, frame, half), BF),
            pltpu.VMEM((n_core, block, half), BF),
            pltpu.VMEM((n_core,) + args[3].shape, F32),
            pltpu.VMEM((3, n_core, block), jnp.int32),
            pltpu.VMEM((frame, half), F32),
            pltpu.VMEM((block, channels), BF),
            pltpu.VMEM((block, width), BF),
            pltpu.VMEM((1, width), F32),
            pltpu.VMEM((block, width), F32),
            pltpu.VMEM((nz, topk, block), jnp.int32),
            pltpu.VMEM((nz, topk, block), F32),
            pltpu.VMEM((nz, rows, block), BF),
            pltpu.VMEM((nz, block, rows), BF),
            pltpu.VMEM((nz, block, main), BF),
            pltpu.VMEM((nz, rows - cap, main), BF),
            pltpu.VMEM((nz, rows, width), BF),
            pltpu.VMEM((rows, ff), BF),
            pltpu.VMEM((nz, rows, main), BF),
            pltpu.VMEM((nz - 1, block, main), BF),
            pltpu.VMEM((nz + 1, block, main), BF),
            pltpu.VMEM((n_plane, topk, block), jnp.int32),
            pltpu.VMEM((n_plane, topk, block), F32),
            pltpu.VMEM((n_plane, nz * n_core * cap, block), BF),
            pltpu.VMEM((n_plane, block, nz * n_core * cap), BF),
            pltpu.VMEM((n_plane, block, slab), BF),
            pltpu.VMEM((nz * n_core, lot, slab), BF),
            pltpu.VMEM((nz * n_core, lot, slab), BF),
            pltpu.VMEM((n_plane, block, slab), BF),
            pltpu.VMEM((n_plane, block, slab), BF),
            dma((12,)), dma((3,)), dma((3,)), dma((2,)), dma((1,)),
            dma((1,)), dma((1,)), dma((2,)), dma((2,)),
            dma((1,)), dma((nz, nc)), dma((1,)), dma((nz,)), dma((1,)), dma((nz, nc)),
            dma((1,)), dma((nz + 1, nc)),
            dma((1,)), dma((1,)), dma((1,)), dma((nz,)), dma((1,)), dma((1,)), dma((1,)), dma((1,)),
        ],
        compiler_params=pltpu.CompilerParams(
            collective_id=0, has_side_effects=True, vmem_limit_bytes=62 * 2**20),
        name="mixer_experts",
    )(*args)


def per_device(
    conv_in, gate_outer, gate_inner, tap_weights, doc_ids, w_proj, stream, norm_gain,
    routes, route_weights, w_gate, w_up, w_down,
):
    n_seq = lax.axis_size("sp")
    n_core = lax.axis_size("tp")
    tok_dev = conv_in.shape[0]
    topk = routes.shape[1]
    capacity = max(2, 2 * tok_dev * topk // (n_core * n_seq * n_core))
    capacity = -(-capacity // 16) * 16
    nz = max(d for d in range(1, math.isqrt(n_seq) + 1) if n_seq % d == 0)
    return layer(
        n_seq, nz, n_seq // nz, n_core, capacity,
        conv_in, gate_outer, gate_inner, tap_weights,
        doc_ids.reshape(n_core, tok_dev // n_core), w_proj, stream, norm_gain.reshape(1, -1),
        routes.T, route_weights.T, w_gate[0], w_up[0], w_down[0])


def solution(mesh):
    in_specs = (
        P("sp", "tp"),
        P("sp", "tp"),
        P("sp", "tp"),
        P(None, "tp"),
        P("sp"),
        P(),
        P(("sp", "tp"), None),
        P(),
        P(("sp", "tp"), None),
        P(("sp", "tp"), None),
        P(("sp", "tp"), None, None),
        P(("sp", "tp"), None, None),
        P(("sp", "tp"), None, None),
    )
    return jax.shard_map(
        per_device, mesh=mesh, in_specs=in_specs, out_specs=P(("sp", "tp"), None), check_vma=False
    )
```

```python
import functools
import math

import jax
import jax.numpy as jnp
from jax import lax
from jax.experimental import pallas as pl
from jax.experimental.pallas import tpu as pltpu
from jax.sharding import PartitionSpec as P

MESH = pl.DeviceIdType.MESH
HALO = 16
SLAB = 512
CHUNKS = 3
BF = jnp.bfloat16
F32 = jnp.float32


def dot(a, b):
    return jnp.dot(a, b, preferred_element_type=F32)


def tile_of(size, most):
    return next(t for t in range(most, 0, -128) if size % t == 0)


def nearest_first(nz):
    return [sorted(range(nz), key=lambda b: (abs(b - z), abs(2 * b - nz + 1) * (1 if nz > 2 else 0), b))
            for z in range(nz)]


def layer_kernel(
    n_seq, nz, n_plane, n_core, cap, cuts, slab,
    ci_hbm, go_hbm, gi_hbm, taps_hbm, docs_hbm, wp_hbm, stream_hbm, gain_hbm,
    routes_hbm, rw_hbm, wg_hbm, wu_hbm, wd_hbm,
    out_ref,
    wg, wu, wd, wp, raw, frames, go_f, taps_f, docs, prod, mixed, stream, gain, hidden,
    rbuf, wbuf, select, spread, zbuf, outgoing, arrived, act, returned, partial, chain,
    rbuf2, wbuf2, select2, spread2, pslab, outgoing2, returned2, partial2, summed2,
    l_sem, e_send, e_recv, h_send, h_recv, d_send, d_recv, rt_send, rt_recv,
    z_send, z_recv, a_send, a_recv, r_send, r_recv, p_send, p_recv,
    s_send, s_recv, v_send, v_recv, w_send, w_recv, f_send, f_recv,
):
    peers = n_plane * n_core
    rows = peers * cap
    block, width = hidden.shape
    ff = wg.shape[1]
    half = ci_hbm.shape[1]
    span = block + HALO
    main = width - slab
    nc = len(cuts)
    wide_col = tile_of(width, 512)
    me = lax.axis_index("sp")
    core = lax.axis_index("tp")
    z, p = me // n_plane, lax.rem(me, n_plane)
    rank = p * n_core + core
    other = 1 - core

    def at_z(b):
        return {"sp": b * n_plane + p, "tp": core}

    def in_plane(q):
        return {"sp": z * n_plane + q, "tp": core}

    def plane_peer(j):
        q = lax.rem(rank + j, peers)
        return {"sp": z * n_plane + q // n_core, "tp": lax.rem(q, n_core)}

    nxt, prv = me + 1, me - 1
    order = nearest_first(nz)

    def ordered(k):
        total = jnp.int32(0)
        for i in range(nz):
            total = total + jnp.where(z == i, order[i][k], 0)
        return total

    def remote(src, dst, send, recv, to):
        return pltpu.make_async_remote_copy(
            src_ref=src, dst_ref=dst, send_sem=send, recv_sem=recv,
            device_id=to, device_id_type=MESH)

    mine = pl.multiple_of(core * (block - HALO), HALO)
    theirs = pl.multiple_of(other * (block - HALO), HALO)
    my_at = pl.multiple_of(other * HALO, HALO)
    their_at = pl.multiple_of(core * HALO, HALO)

    def local(i, src, dst):
        return pltpu.make_async_copy(src, dst, l_sem.at[i])

    hbm_in = (ci_hbm, gi_hbm)
    front = [
        local(0, src.at[pl.ds(mine, span)], frames.at[i, core, pl.ds(my_at, span)]) for i, src in enumerate(hbm_in)
    ] + [
        local(1, go_hbm.at[pl.ds(pl.multiple_of(core * block, HALO), block)], go_f.at[core]),
        local(2, taps_hbm, taps_f.at[core]),
        local(3, stream_hbm, stream),
        local(4, gain_hbm, gain),
    ]
    own_frames = frames.at[:, core, pl.ds(my_at, span)]
    front_waits = [pltpu.make_async_copy(own_frames, own_frames, l_sem.at[0])] + front[2:]
    papers = local(5, docs_hbm, docs.at[0])
    stage = [local(6, src, raw.at[i]) for i, src in enumerate((ci_hbm, gi_hbm, go_hbm))]
    stage_wait = pltpu.make_async_copy(raw, raw, l_sem.at[6])
    tables = [local(7, routes_hbm, rbuf.at[z]), local(7, rw_hbm, wbuf.at[z]),
              local(7, routes_hbm, rbuf2.at[p]), local(7, rw_hbm, wbuf2.at[p])]
    topk = routes_hbm.shape[0]

    def lists_of(count):
        return hidden.at[pl.ds(0, 2 * topk), pl.ds(0, count * block)]

    tables_wait = pltpu.make_async_copy(lists_of(2), lists_of(2), l_sem.at[7])
    project = local(8, wp_hbm, wp)
    weights = [local(9, wg_hbm, wg), local(10, wu_hbm, wu), local(11, wd_hbm, wd)]
    for load in stage + [papers] + front + tables:
        load.start()

    barrier = pltpu.get_barrier_semaphore()

    def greet(to):
        pl.semaphore_signal(barrier, inc=1, device_id=to, device_id_type=MESH)

    for k in range(1, nz):
        greet(at_z(lax.rem(z + k, nz)))
        greet({"sp": lax.rem(z + k, nz) * n_plane + p, "tp": other})
    for j in range(1, peers):
        greet(plane_peer(j))
    has_prv, has_nxt = me > 0, me < n_seq - 1
    for n, there in ((nxt, has_nxt), (prv, has_prv)):
        @pl.when(there)
        def _():
            for c in range(n_core):
                greet({"sp": n, "tp": jnp.int32(c)})
    sides = jnp.where(has_prv, n_core, 0) + jnp.where(has_nxt, n_core, 0)
    pl.semaphore_wait(barrier, 2 * (nz - 1) + peers - 1 + sides)

    edge = ci_hbm.shape[0] - HALO
    far = block + HALO
    partner = {"tp": other}
    to_next = [
        remote(raw.at[i, pl.ds(edge, HALO)], frames.at[i, core, pl.ds(0, HALO)],
               h_send.at[0], h_recv.at[0], {"sp": nxt, "tp": jnp.int32(0)}) for i in range(2)]
    to_prev = [
        remote(raw.at[i, pl.ds(0, HALO)], frames.at[i, core, pl.ds(far, HALO)],
               h_send.at[1], h_recv.at[0], {"sp": prv, "tp": jnp.int32(1)}) for i in range(2)]
    halo_part = frames.at[:, core, pl.ds(0, HALO)]
    docs_next = remote(docs.at[0], docs.at[1], d_send.at[0], d_recv.at[0], {"sp": nxt, "tp": core})
    docs_prev = remote(docs.at[0], docs.at[2], d_send.at[0], d_recv.at[0], {"sp": prv, "tp": core})
    first_half = core == 0
    inside = (first_half & has_prv) | (jnp.logical_not(first_half) & has_nxt)
    swaps = [
        remote(raw.at[i, pl.ds(theirs, span)], frames.at[i, core, pl.ds(their_at, span)],
               e_send.at[0], e_recv.at[0], partner) for i in range(2)
    ] + [
        remote(raw.at[2, pl.ds(pl.multiple_of(other * block, HALO), block)], go_f.at[core],
               e_send.at[1], e_recv.at[1], partner),
        remote(taps_hbm, taps_f.at[core], e_send.at[2], e_recv.at[2], partner),
    ]
    their_frames = frames.at[:, core, pl.ds(their_at, span)]
    swap_waits = [remote(their_frames, their_frames, e_send.at[0], e_recv.at[0], partner)] + swaps[2:]
    stage_wait.wait()
    papers.wait()
    for copies, there in ((to_next, has_nxt), (to_prev, has_prv)):
        @pl.when(there)
        def _():
            for copy in copies:
                copy.start()

    @pl.when(first_half & has_nxt)
    def _():
        docs_next.start()

    @pl.when(jnp.logical_not(first_half) & has_prv)
    def _():
        docs_prev.start()

    for copy in swaps:
        copy.start()
    project.start()
    lists = []
    for k in range(1, nz):
        to = at_z(lax.rem(z + k, nz))
        lists.append(remote(routes_hbm, rbuf.at[z], rt_send.at[0], rt_recv.at[0], to))
        lists.append(remote(rw_hbm, wbuf.at[z], rt_send.at[0], rt_recv.at[0], to))
    for i in range(1, n_plane):
        to = in_plane(lax.rem(p + i, n_plane))
        lists.append(remote(routes_hbm, rbuf2.at[p], rt_send.at[1], rt_recv.at[1], to))
        lists.append(remote(rw_hbm, wbuf2.at[p], rt_send.at[1], rt_recv.at[1], to))
    for copy in lists:
        copy.start()
    list_waits = [
        remote(lists_of(n - 1), lists_of(n - 1), rt_send.at[i], rt_recv.at[i], partner)
        for i, n in enumerate((nz, n_plane))
    ]

    lane = lax.broadcasted_iota(jnp.int32, (block, block), 1)
    sub = lax.broadcasted_iota(jnp.int32, (block, block), 0)
    below = (sub < lane).astype(BF)

    def slots(chosen, weight, expert, put):
        count = expert.shape[0]
        named = jnp.zeros((count, block), F32)
        share = jnp.zeros((count, block), F32)
        for i in range(chosen.shape[0]):
            hit = jnp.broadcast_to(chosen[i:i + 1], (count, block)) == expert
            named = jnp.where(hit, 1.0, named)
            share = jnp.where(hit, jnp.broadcast_to(weight[i:i + 1], (count, block)), share)
        place = dot(named.astype(BF), below)
        place = jnp.where(named > 0.0, place, -1.0)
        seat = lax.broadcasted_iota(jnp.int32, (cap, block), 0).astype(F32)
        chosen_rows, pieces = [], []
        for j in range(count):
            here = jnp.broadcast_to(place[j:j + 1], (cap, block)) == seat
            chosen_rows.append(jnp.where(here, 1.0, 0.0).astype(BF))
            pieces.append(jnp.where(here, jnp.broadcast_to(share[j:j + 1], (cap, block)), 0.0))
        put(jnp.concatenate(chosen_rows, axis=0), jnp.concatenate(pieces, axis=0).T.astype(BF))

    def line_slots(k):
        b = ordered(k)
        group = lax.broadcasted_iota(jnp.int32, (peers, block), 0)

        def put(pick, share):
            select[k] = pick
            spread[k] = share

        slots(rbuf[b], wbuf[b], z * peers + lax.rem(rank + group, peers), put)

    def plane_slots(q):
        group = lax.broadcasted_iota(jnp.int32, (nz * n_core, block), 0)

        def put(pick, share):
            select2[q] = pick
            spread2[q] = share

        slots(rbuf2[q], wbuf2[q], group // n_core * peers + p * n_core + lax.rem(group, n_core), put)

    tables_wait.wait()
    line_slots(0)

    for load in front_waits:
        load.wait()
    for copy in swap_waits:
        copy.wait_recv()

    halo_at = pl.ds(pl.multiple_of(core * far, HALO), HALO)

    @pl.when(inside)
    def _():
        docs_next.wait_recv()
        here = frames.at[:, :, halo_at]
        remote(here, here, h_send.at[0], h_recv.at[0], partner).wait_recv()

    @pl.when(jnp.logical_not(inside))
    def _():
        for h in range(n_core):
            for i in range(2):
                frames[i, h, halo_at, :] = jnp.zeros((HALO, half), BF)

    @pl.when(jnp.logical_not(first_half & has_prv))
    def _():
        docs[1] = docs[0]

    @pl.when(first_half | jnp.logical_not(has_nxt))
    def _():
        docs[2] = docs[0]

    for load in weights:
        load.start()

    own, before_docs, after_docs = docs[0], docs[1], docs[2]
    wide = (8, block)

    def row(x):
        return jnp.broadcast_to(x.astype(F32), wide)

    cur = row(jnp.where(first_half, own[0:1], own[1:2]))
    left = row(jnp.where(first_half, before_docs[1:2], own[0:1]))
    right = row(jnp.where(first_half, own[1:2], after_docs[0:1]))
    lanes = lax.broadcasted_iota(jnp.int32, wide, 1)
    before = jnp.where(lanes == 0, pltpu.roll(left, 1, 1), pltpu.roll(cur, 1, 1))
    after = jnp.where(lanes == block - 1, pltpu.roll(right, block - 1, 1), pltpu.roll(cur, block - 1, 1))
    position = (me * n_core + core) * block + lanes
    has_before = (cur == before) & (position > 0)
    has_after = (cur == after) & (position < n_seq * n_core * block - 1)
    both = jnp.where(lax.broadcasted_iota(jnp.int32, wide, 0) == 0,
                     jnp.where(has_before, 1.0, 0.0), jnp.where(has_after, 1.0, 0.0))
    marks = jnp.concatenate([both] * (block // 8), axis=0).T
    keep_before, keep_after = marks[:, 0:1], marks[:, 1:2]

    for h in range(n_core):
        prod[...] = frames[1, h].astype(F32) * frames[0, h].astype(F32)
        conv = (
            taps_f[h, 0:1, :] * (prod[HALO - 1:HALO - 1 + block, :] * keep_before)
            + taps_f[h, 1:2, :] * prod[HALO:HALO + block, :]
            + taps_f[h, 2:3, :] * (prod[HALO + 1:HALO + 1 + block, :] * keep_after)
        )
        mixed[:, h * half:(h + 1) * half] = (go_f[h].astype(F32) * conv).astype(BF)

    project.wait()
    square = jnp.zeros((block, 128), F32)
    for q in range(width // wide_col):
        cols = slice(q * wide_col, (q + 1) * wide_col)
        value = stream[:, cols].astype(F32) + dot(mixed[...], wp[:, cols])
        hidden[:, cols] = value
        value = value * value
        for i in range(wide_col // 128):
            square = square + value[:, i * 128:(i + 1) * 128]
    scale = lax.rsqrt(jnp.sum(square, axis=1, keepdims=True) / width + 1e-05)

    def chunk(q):
        return pl.ds(*cuts[q])

    def z_up(h, q):
        b = z - h
        piece = zbuf.at[b, :, chunk(q)]
        return remote(piece, piece, z_send.at[0], z_recv.at[b, q], at_z(z + 1))

    def z_down(h, q):
        b = z + h
        piece = zbuf.at[b, :, chunk(q)]
        return remote(piece, piece, z_send.at[0], z_recv.at[b, q], at_z(z - 1))

    def normed(cols):
        return (hidden[:, cols] * scale * gain[:, cols]).astype(BF)

    side = slice(main, width)
    pslab[p] = normed(side)
    s_copies = [
        remote(pslab.at[p], pslab.at[p], s_send.at[0], s_recv.at[0], in_plane(lax.rem(p + i, n_plane)))
        for i in range(1, n_plane)
    ]
    for copy in s_copies:
        copy.start()
    for q in range(nc):
        zbuf[z, :, chunk(q)] = normed(chunk(q))

    for q in range(nc):
        @pl.when(z < nz - 1)
        def _():
            z_up(0, q).start()

        @pl.when(z > 0)
        def _():
            z_down(0, q).start()

    def pump(h, q):
        @pl.when(z >= h)
        def _():
            piece = zbuf.at[z - h, :, chunk(q)]
            remote(piece, piece, z_send.at[0], z_recv.at[z - h, q], at_z(z)).wait_recv()

            @pl.when(z < nz - 1)
            def _():
                z_up(h, q).start()

        @pl.when(z + h < nz)
        def _():
            piece = zbuf.at[z + h, :, chunk(q)]
            remote(piece, piece, z_send.at[0], z_recv.at[z + h, q], at_z(z)).wait_recv()

            @pl.when(z > 0)
            def _():
                z_down(h, q).start()

    def seat_of(source):
        return pl.multiple_of((lax.rem(source, n_core) * n_plane + source // n_core) * cap, HALO)

    my_seat = seat_of(rank)

    def a_copy(k, j, q):
        b = ordered(k)
        return remote(
            outgoing.at[k, pl.ds((j - 1) * cap, cap), chunk(q)], arrived.at[b, pl.ds(my_seat, cap), chunk(q)],
            a_send.at[0], a_recv.at[b], plane_peer(j))

    def a_all(k):
        b = ordered(k)
        return remote(outgoing.at[k], arrived.at[b, pl.ds(cap, rows - cap), pl.ds(0, main)],
                      a_send.at[0], a_recv.at[b], plane_peer(1))

    def r_copy(k, j, q):
        b = ordered(k)
        seat = seat_of(lax.rem(rank + peers - j, peers))
        return remote(
            arrived.at[b, pl.ds(seat, cap), chunk(q)], returned.at[b, pl.ds(j * cap, cap), chunk(q)],
            r_send.at[0], r_recv.at[b, q], plane_peer(peers - j))

    def r_all(k, q):
        b = ordered(k)
        return remote(
            arrived.at[b, pl.ds(cap, rows - cap), chunk(q)], returned.at[b, pl.ds(cap, rows - cap), chunk(q)],
            r_send.at[0], r_recv.at[b, q], plane_peer(1))

    def dispatch(k):
        b = ordered(k)

        for q in range(nc):
            if k:
                pump(k, q)
            cols = chunk(q)
            picked = dot(select[k], zbuf[b, :, cols]).astype(BF)
            arrived[b, pl.ds(my_seat, cap), cols] = picked[:cap]
            outgoing[k, :, cols] = picked[cap:]
            for j in range(1, peers):
                a_copy(k, j, q).start()

    lot = n_plane * cap
    side_ref = pl.ds(main, slab)
    my_lot = pl.multiple_of(core * lot, HALO)
    other_lot = pl.multiple_of(other * lot, HALO)

    def v_copy(b, c):
        return remote(
            outgoing2.at[b * n_core + c], arrived.at[z, pl.ds(my_lot, lot), side_ref],
            v_send.at[0], v_recv.at[z], {"sp": b * n_plane + p, "tp": c})

    def v_wait(b, count):
        piece = arrived.at[b, pl.ds(0, count * lot), side_ref]
        remote(piece, piece, v_send.at[0], v_recv.at[b], partner).wait_recv()

    def rest(ref):
        return ref.at[pl.ds(0, ref.shape[0] - 1)]

    def all_of(ref, send, recv):
        return remote(ref, ref, send, recv, partner)

    s_all = all_of(rest(pslab), s_send.at[0], s_recv.at[0])
    v_all = all_of(rest(outgoing2), v_send.at[0], v_recv.at[0])
    w_all = all_of(rest(returned2), w_send.at[0], w_recv.at[0])
    f_all = all_of(rest(partial2), f_send.at[0], f_recv.at[0])

    def side_pick():
        s_all.wait_recv()
        for q in range(n_plane):
            plane_slots(q)
            picked = dot(select2[q], pslab[q]).astype(BF)
            for b in range(nz):
                for c in range(n_core):
                    at = (b * n_core + c) * cap
                    outgoing2[b * n_core + c, q * cap:(q + 1) * cap, :] = picked[at:at + cap]
        arrived[z, pl.ds(my_lot, lot), side] = outgoing2[z * n_core + core]
        v_copy(z, other).start()

    def side_send(h):
        @pl.when(z + h < nz)
        def _():
            for c in range(n_core):
                v_copy(z + h, jnp.int32(c)).start()

        @pl.when(z >= h)
        def _():
            for c in range(n_core):
                v_copy(z - h, jnp.int32(c)).start()

    def w_copy(b, c):
        piece = arrived.at[b, pl.ds(pl.multiple_of(c * lot, HALO), lot), side_ref]
        return remote(piece, returned2.at[z * n_core + core], w_send.at[0], w_recv.at[0],
                      {"sp": b * n_plane + p, "tp": c})

    def f_copy(q):
        return remote(partial2.at[q], summed2.at[p], f_send.at[0], f_recv.at[0], in_plane(q))

    def side_combine():
        w_all.wait_recv()
        for q in range(n_plane):
            results = jnp.concatenate(
                [returned2[b, q * cap:(q + 1) * cap, :] for b in range(nz * n_core)], axis=0)
            total = dot(spread2[q], results)

            @pl.when(p == q)
            def _():
                hidden[:, side] = hidden[:, side] + total

            @pl.when(p != q)
            def _():
                partial2[q] = total.astype(BF)
                f_copy(jnp.int32(q)).start()

    fcol = tile_of(ff, 256)

    def expert(k):
        b = ordered(k)
        if k == 0:
            for load in weights:
                load.wait()
            v_wait(z, n_core - 1)
        else:
            v_wait(b, n_core)

        a_all(k).wait_recv()

        @pl.loop(0, ff // fcol)
        def _(i):
            cols = pl.ds(pl.multiple_of(i * fcol, fcol), fcol)
            gate = jnp.minimum(dot(arrived[b], wg[:, cols]), 7.0)
            upper = jnp.clip(dot(arrived[b], wu[:, cols]), -7.0, 7.0)
            act[:, cols] = ((upper + 1.0) * gate * jax.nn.sigmoid(1.702 * gate)).astype(BF)

        arrived[b, :, side] = dot(act[...], wd[:, side]).astype(BF)
        if k == 0:
            returned2[z * n_core + core] = arrived[z, pl.ds(my_lot, lot), side]
            w_copy(z, other).start()
        else:
            for c in range(n_core):
                w_copy(b, c).start()

        for q in range(nc):
            cols = chunk(q)
            arrived[b, :, cols] = dot(act[...], wd[:, cols]).astype(BF)
            returned[b, 0:cap, cols] = arrived[b, pl.ds(my_seat, cap), cols]
            if k == nz - 1:
                give(k, q)

    def give(k, q):
        for j in range(1, peers):
            r_copy(k, j, q).start()

    def chained(b):
        return ((b < z) & (z < nz - 1)) | ((b > z) & (z > 0))

    def p_copy(k, q):
        b = ordered(k)
        down = b < z
        seat = jnp.where(down & (b == z - 1), nz, b)
        return remote(partial.at[k - 1, :, chunk(q)], chain.at[seat, :, chunk(q)],
                      p_send.at[0], p_recv.at[seat, q], at_z(jnp.where(down, z - 1, z + 1)))

    def p_wait(seat, q):
        piece = chain.at[seat, :, chunk(q)]
        remote(piece, piece, p_send.at[0], p_recv.at[seat, q], at_z(z)).wait_recv()

    def combine(k):
        b = ordered(k)

        for q in range(nc):
            cols = chunk(q)
            r_all(k, q).wait_recv()
            total = dot(spread[k], returned[b, :, cols])
            if k == 0:
                hidden[:, cols] = hidden[:, cols] + total
            else:
                @pl.when(chained(b))
                def _():
                    p_wait(b, q)
                    partial[k - 1, :, cols] = (total + chain[b, :, cols].astype(F32)).astype(BF)

                @pl.when(jnp.logical_not(chained(b)))
                def _():
                    partial[k - 1, :, cols] = total.astype(BF)

                p_copy(k, q).start()

    def give_all(k, low, high):
        for q in range(low, high):
            give(k, q)

    dispatch(0)
    for copy in list_waits:
        copy.wait_recv()
    for k in range(1, nz):
        line_slots(k)
        if k == nz - 1:
            give_all(0, 0, nc // 2)
        dispatch(k)
        if k == 1:
            side_pick()
        side_send(k)
        if k < nz - 1:
            expert(k - 1)
    give_all(0, nc // 2, nc)
    expert(nz - 2)
    expert(nz - 1)
    for k in range(nz - 2, 0, -1):
        give_all(k, 0, nc)
    combine(nz - 1)
    side_combine()
    for k in range(nz - 2, -1, -1):
        combine(k)
    f_all.wait_recv()
    for q in range(n_plane):
        @pl.when(p != q)
        def _():
            hidden[:, side] = hidden[:, side] + summed2[q].astype(F32)
    out_ref[:, side] = hidden[:, side].astype(BF)

    for q in range(nc):
        cols = chunk(q)

        @pl.when(z > 0)
        def _():
            p_wait(z, q)
            hidden[:, cols] = hidden[:, cols] + chain[z, :, cols].astype(F32)

        @pl.when(z < nz - 1)
        def _():
            p_wait(nz, q)
            hidden[:, cols] = hidden[:, cols] + chain[nz, :, cols].astype(F32)

        out_ref[:, cols] = hidden[:, cols].astype(BF)

    for i, there in enumerate((has_nxt, has_prv)):
        @pl.when(there)
        def _():
            remote(halo_part, halo_part, h_send.at[i], h_recv.at[0], partner).wait_send()

    @pl.when((first_half & has_nxt) | (jnp.logical_not(first_half) & has_prv))
    def _():
        docs_next.wait_send()

    for copy in swap_waits + list_waits + [s_all, v_all, w_all, f_all]:
        copy.wait_send()
    middle = (z > 0) & (z < nz - 1)

    @pl.when(middle)
    def _():
        remote(chain, chain, z_send.at[0], z_recv.at[0, 0], partner).wait_send()

    @pl.when(jnp.logical_not(middle))
    def _():
        remote(chain.at[0], chain.at[0], z_send.at[0], z_recv.at[0, 0], partner).wait_send()

    remote(outgoing, outgoing, a_send.at[0], a_recv.at[0], partner).wait_send()
    remote(outgoing, outgoing, r_send.at[0], r_recv.at[0, 0], partner).wait_send()
    remote(partial, partial, p_send.at[0], p_recv.at[0, 0], partner).wait_send()


def layer(n_seq, nz, n_plane, n_core, cap, *args):
    tok, half = args[0].shape
    block, width = args[6].shape
    ff = args[10].shape[1]
    peers = n_plane * n_core
    rows = peers * cap
    topk = args[8].shape[0]
    channels = half * n_core
    frame = block + 2 * HALO
    slab = SLAB if width > 2 * SLAB else 128
    main = width - slab
    parts = main // 128
    nc = min(CHUNKS, parts)
    edges = [-(-parts * i // nc) * 128 for i in range(nc + 1)]
    cuts = [(a, b - a) for a, b in zip(edges, edges[1:])]
    lot = n_plane * cap
    hbm = pl.BlockSpec(memory_space=pl.ANY)
    vmem = pl.BlockSpec(memory_space=pltpu.VMEM)
    dma = pltpu.SemaphoreType.DMA
    return pl.pallas_call(
        functools.partial(layer_kernel, n_seq, nz, n_plane, n_core, cap, cuts, slab),
        out_shape=jax.ShapeDtypeStruct((block, width), BF),
        in_specs=[hbm] * len(args),
        out_specs=vmem,
        scratch_shapes=[
            pltpu.VMEM((width, ff), BF),
            pltpu.VMEM((width, ff), BF),
            pltpu.VMEM((ff, width), BF),
            pltpu.VMEM((channels, width), BF),
            pltpu.VMEM((3, tok, half), BF),
            pltpu.VMEM((2, n_core, frame, half), BF),
            pltpu.VMEM((n_core, block, half), BF),
            pltpu.VMEM((n_core,) + args[3].shape, F32),
            pltpu.VMEM((3, n_core, block), jnp.int32),
            pltpu.VMEM((frame, half), F32),
            pltpu.VMEM((block, channels), BF),
            pltpu.VMEM((block, width), BF),
            pltpu.VMEM((1, width), F32),
            pltpu.VMEM((block, width), F32),
            pltpu.VMEM((nz, topk, block), jnp.int32),
            pltpu.VMEM((nz, topk, block), F32),
            pltpu.VMEM((nz, rows, block), BF),
            pltpu.VMEM((nz, block, rows), BF),
            pltpu.VMEM((nz, block, main), BF),
            pltpu.VMEM((nz, rows - cap, main), BF),
            pltpu.VMEM((nz, rows, width), BF),
            pltpu.VMEM((rows, ff), BF),
            pltpu.VMEM((nz, rows, main), BF),
            pltpu.VMEM((nz - 1, block, main), BF),
            pltpu.VMEM((nz + 1, block, main), BF),
            pltpu.VMEM((n_plane, topk, block), jnp.int32),
            pltpu.VMEM((n_plane, topk, block), F32),
            pltpu.VMEM((n_plane, nz * n_core * cap, block), BF),
            pltpu.VMEM((n_plane, block, nz * n_core * cap), BF),
            pltpu.VMEM((n_plane, block, slab), BF),
            pltpu.VMEM((nz * n_core, lot, slab), BF),
            pltpu.VMEM((nz * n_core, lot, slab), BF),
            pltpu.VMEM((n_plane, block, slab), BF),
            pltpu.VMEM((n_plane, block, slab), BF),
            dma((12,)), dma((3,)), dma((3,)), dma((2,)), dma((1,)),
            dma((1,)), dma((1,)), dma((2,)), dma((2,)),
            dma((1,)), dma((nz, nc)), dma((1,)), dma((nz,)), dma((1,)), dma((nz, nc)),
            dma((1,)), dma((nz + 1, nc)),
            dma((1,)), dma((1,)), dma((1,)), dma((nz,)), dma((1,)), dma((1,)), dma((1,)), dma((1,)),
        ],
        compiler_params=pltpu.CompilerParams(
            collective_id=0, has_side_effects=True, vmem_limit_bytes=62 * 2**20),
        name="mixer_experts",
    )(*args)


def per_device(
    conv_in, gate_outer, gate_inner, tap_weights, doc_ids, w_proj, stream, norm_gain,
    routes, route_weights, w_gate, w_up, w_down,
):
    n_seq = lax.axis_size("sp")
    n_core = lax.axis_size("tp")
    tok_dev = conv_in.shape[0]
    topk = routes.shape[1]
    capacity = max(2, 2 * tok_dev * topk // (n_core * n_seq * n_core))
    capacity = -(-capacity // 16) * 16
    nz = max(d for d in range(1, math.isqrt(n_seq) + 1) if n_seq % d == 0)
    return layer(
        n_seq, nz, n_seq // nz, n_core, capacity,
        conv_in, gate_outer, gate_inner, tap_weights,
        doc_ids.reshape(n_core, tok_dev // n_core), w_proj, stream, norm_gain.reshape(1, -1),
        routes.T, route_weights.T, w_gate[0], w_up[0], w_down[0])


def solution(mesh):
    in_specs = (
        P("sp", "tp"),
        P("sp", "tp"),
        P("sp", "tp"),
        P(None, "tp"),
        P("sp"),
        P(),
        P(("sp", "tp"), None),
        P(),
        P(("sp", "tp"), None),
        P(("sp", "tp"), None),
        P(("sp", "tp"), None, None),
        P(("sp", "tp"), None, None),
        P(("sp", "tp"), None, None),
    )
    return jax.shard_map(
        per_device, mesh=mesh, in_specs=in_specs, out_specs=P(("sp", "tp"), None), check_vma=False
    )
```

```python
import functools
import math

import jax
import jax.numpy as jnp
from jax import lax
from jax.experimental import pallas as pl
from jax.experimental.pallas import tpu as pltpu
from jax.sharding import PartitionSpec as P

MESH = pl.DeviceIdType.MESH
HALO = 16
SLAB = 512
CHUNKS = 3
BF = jnp.bfloat16
F32 = jnp.float32


def dot(a, b):
    return jnp.dot(a, b, preferred_element_type=F32)


def tile_of(size, most):
    return next(t for t in range(most, 0, -128) if size % t == 0)


def nearest_first(nz):
    return [sorted(range(nz), key=lambda b: (abs(b - z), abs(2 * b - nz + 1) * (1 if nz > 2 else 0), b))
            for z in range(nz)]


def layer_kernel(
    n_seq, nz, n_plane, n_core, cap, cuts, slab,
    ci_hbm, go_hbm, gi_hbm, taps_hbm, docs_hbm, wp_hbm, stream_hbm, gain_hbm,
    routes_hbm, rw_hbm, wg_hbm, wu_hbm, wd_hbm,
    out_ref,
    wg, wu, wd, wp, raw, frames, go_f, taps_f, docs, prod, mixed, stream, gain, hidden,
    rbuf, wbuf, select, spread, zbuf, outgoing, arrived, act, returned, partial, chain,
    early, rbuf2, wbuf2, select2, spread2, pslab, outgoing2, returned2, partial2, summed2,
    l_sem, e_send, e_recv, h_send, h_recv, d_send, d_recv, rt_send, rt_recv,
    z_send, z_recv, a_send, a_recv, r_send, r_recv, p_send, p_recv,
    s_send, s_recv, v_send, v_recv, w_send, w_recv, f_send, f_recv,
):
    peers = n_plane * n_core
    rows = peers * cap
    block, width = hidden.shape
    ff = wg.shape[1]
    half = ci_hbm.shape[1]
    span = block + HALO
    main = width - slab
    nc = len(cuts)
    wide_col = tile_of(width, 512)
    me = lax.axis_index("sp")
    core = lax.axis_index("tp")
    z, p = me // n_plane, lax.rem(me, n_plane)
    rank = p * n_core + core
    other = 1 - core

    def at_z(b):
        return {"sp": b * n_plane + p, "tp": core}

    def in_plane(q):
        return {"sp": z * n_plane + q, "tp": core}

    def plane_peer(j):
        q = lax.rem(rank + j, peers)
        return {"sp": z * n_plane + q // n_core, "tp": lax.rem(q, n_core)}

    nxt, prv = me + 1, me - 1
    order = nearest_first(nz)

    def ordered(k):
        total = jnp.int32(0)
        for i in range(nz):
            total = total + jnp.where(z == i, order[i][k], 0)
        return total

    def remote(src, dst, send, recv, to):
        return pltpu.make_async_remote_copy(
            src_ref=src, dst_ref=dst, send_sem=send, recv_sem=recv,
            device_id=to, device_id_type=MESH)

    mine = pl.multiple_of(core * (block - HALO), HALO)
    theirs = pl.multiple_of(other * (block - HALO), HALO)
    my_at = pl.multiple_of(other * HALO, HALO)
    their_at = pl.multiple_of(core * HALO, HALO)

    def local(i, src, dst):
        return pltpu.make_async_copy(src, dst, l_sem.at[i])

    hbm_in = (ci_hbm, gi_hbm)
    front = [
        local(0, src.at[pl.ds(mine, span)], frames.at[i, core, pl.ds(my_at, span)]) for i, src in enumerate(hbm_in)
    ] + [
        local(1, go_hbm.at[pl.ds(pl.multiple_of(core * block, HALO), block)], go_f.at[core]),
        local(2, taps_hbm, taps_f.at[core]),
        local(3, stream_hbm, stream),
        local(4, gain_hbm, gain),
    ]
    own_frames = frames.at[:, core, pl.ds(my_at, span)]
    front_waits = [pltpu.make_async_copy(own_frames, own_frames, l_sem.at[0])] + front[2:]
    papers = local(5, docs_hbm, docs.at[0])
    stage = [local(6, src, raw.at[i]) for i, src in enumerate((ci_hbm, gi_hbm, go_hbm))]
    stage_wait = pltpu.make_async_copy(raw, raw, l_sem.at[6])
    tables = [local(7, routes_hbm, rbuf.at[z]), local(7, rw_hbm, wbuf.at[z]),
              local(7, routes_hbm, rbuf2.at[p]), local(7, rw_hbm, wbuf2.at[p])]
    topk = routes_hbm.shape[0]

    def lists_of(count):
        return hidden.at[pl.ds(0, 2 * topk), pl.ds(0, count * block)]

    tables_wait = pltpu.make_async_copy(lists_of(2), lists_of(2), l_sem.at[7])
    project = local(8, wp_hbm, wp)
    weights = [local(9, wg_hbm, wg), local(10, wu_hbm, wu), local(11, wd_hbm, wd)]
    for load in stage + [papers] + front + tables:
        load.start()

    barrier = pltpu.get_barrier_semaphore()

    def greet(to):
        pl.semaphore_signal(barrier, inc=1, device_id=to, device_id_type=MESH)

    for k in range(1, nz):
        greet(at_z(lax.rem(z + k, nz)))
        greet({"sp": lax.rem(z + k, nz) * n_plane + p, "tp": other})
    for j in range(1, peers):
        greet(plane_peer(j))
    has_prv, has_nxt = me > 0, me < n_seq - 1
    for n, there in ((nxt, has_nxt), (prv, has_prv)):
        @pl.when(there)
        def _():
            for c in range(n_core):
                greet({"sp": n, "tp": jnp.int32(c)})
    sides = jnp.where(has_prv, n_core, 0) + jnp.where(has_nxt, n_core, 0)
    pl.semaphore_wait(barrier, 2 * (nz - 1) + peers - 1 + sides)

    edge = ci_hbm.shape[0] - HALO
    far = block + HALO
    partner = {"tp": other}
    to_next = [
        remote(raw.at[i, pl.ds(edge, HALO)], frames.at[i, core, pl.ds(0, HALO)],
               h_send.at[0], h_recv.at[0], {"sp": nxt, "tp": jnp.int32(0)}) for i in range(2)]
    to_prev = [
        remote(raw.at[i, pl.ds(0, HALO)], frames.at[i, core, pl.ds(far, HALO)],
               h_send.at[1], h_recv.at[0], {"sp": prv, "tp": jnp.int32(1)}) for i in range(2)]
    halo_part = frames.at[:, core, pl.ds(0, HALO)]
    docs_next = remote(docs.at[0], docs.at[1], d_send.at[0], d_recv.at[0], {"sp": nxt, "tp": core})
    docs_prev = remote(docs.at[0], docs.at[2], d_send.at[0], d_recv.at[0], {"sp": prv, "tp": core})
    first_half = core == 0
    inside = (first_half & has_prv) | (jnp.logical_not(first_half) & has_nxt)
    swaps = [
        remote(raw.at[i, pl.ds(theirs, span)], frames.at[i, core, pl.ds(their_at, span)],
               e_send.at[0], e_recv.at[0], partner) for i in range(2)
    ] + [
        remote(raw.at[2, pl.ds(pl.multiple_of(other * block, HALO), block)], go_f.at[core],
               e_send.at[1], e_recv.at[1], partner),
        remote(taps_hbm, taps_f.at[core], e_send.at[2], e_recv.at[2], partner),
    ]
    their_frames = frames.at[:, core, pl.ds(their_at, span)]
    swap_waits = [remote(their_frames, their_frames, e_send.at[0], e_recv.at[0], partner)] + swaps[2:]
    stage_wait.wait()
    papers.wait()
    for copies, there in ((to_next, has_nxt), (to_prev, has_prv)):
        @pl.when(there)
        def _():
            for copy in copies:
                copy.start()

    @pl.when(first_half & has_nxt)
    def _():
        docs_next.start()

    @pl.when(jnp.logical_not(first_half) & has_prv)
    def _():
        docs_prev.start()

    for copy in swaps:
        copy.start()
    project.start()
    lists = []
    for k in range(1, nz):
        to = at_z(lax.rem(z + k, nz))
        lists.append(remote(routes_hbm, rbuf.at[z], rt_send.at[0], rt_recv.at[0], to))
        lists.append(remote(rw_hbm, wbuf.at[z], rt_send.at[0], rt_recv.at[0], to))
    for i in range(1, n_plane):
        to = in_plane(lax.rem(p + i, n_plane))
        lists.append(remote(routes_hbm, rbuf2.at[p], rt_send.at[1], rt_recv.at[1], to))
        lists.append(remote(rw_hbm, wbuf2.at[p], rt_send.at[1], rt_recv.at[1], to))
    for copy in lists:
        copy.start()
    list_waits = [
        remote(lists_of(n - 1), lists_of(n - 1), rt_send.at[i], rt_recv.at[i], partner)
        for i, n in enumerate((nz, n_plane))
    ]

    lane = lax.broadcasted_iota(jnp.int32, (block, block), 1)
    sub = lax.broadcasted_iota(jnp.int32, (block, block), 0)
    below = (sub < lane).astype(BF)

    def slots(chosen, weight, expert, put):
        count = expert.shape[0]
        named = jnp.zeros((count, block), F32)
        share = jnp.zeros((count, block), F32)
        for i in range(chosen.shape[0]):
            hit = jnp.broadcast_to(chosen[i:i + 1], (count, block)) == expert
            named = jnp.where(hit, 1.0, named)
            share = jnp.where(hit, jnp.broadcast_to(weight[i:i + 1], (count, block)), share)
        place = dot(named.astype(BF), below)
        place = jnp.where(named > 0.0, place, -1.0)
        seat = lax.broadcasted_iota(jnp.int32, (cap, block), 0).astype(F32)
        chosen_rows, pieces = [], []
        for j in range(count):
            here = jnp.broadcast_to(place[j:j + 1], (cap, block)) == seat
            chosen_rows.append(jnp.where(here, 1.0, 0.0).astype(BF))
            pieces.append(jnp.where(here, jnp.broadcast_to(share[j:j + 1], (cap, block)), 0.0))
        put(jnp.concatenate(chosen_rows, axis=0), jnp.concatenate(pieces, axis=0).T.astype(BF))

    def line_slots(k):
        b = ordered(k)
        group = lax.broadcasted_iota(jnp.int32, (peers, block), 0)

        def put(pick, share):
            select[k] = pick
            spread[k] = share

        slots(rbuf[b], wbuf[b], z * peers + lax.rem(rank + group, peers), put)

    def plane_slots(q):
        group = lax.broadcasted_iota(jnp.int32, (nz * n_core, block), 0)

        def put(pick, share):
            select2[q] = pick
            spread2[q] = share

        slots(rbuf2[q], wbuf2[q], group // n_core * peers + p * n_core + lax.rem(group, n_core), put)

    tables_wait.wait()
    line_slots(0)

    for load in front_waits:
        load.wait()
    for copy in swap_waits:
        copy.wait_recv()

    halo_at = pl.ds(pl.multiple_of(core * far, HALO), HALO)

    @pl.when(inside)
    def _():
        docs_next.wait_recv()
        here = frames.at[:, :, halo_at]
        remote(here, here, h_send.at[0], h_recv.at[0], partner).wait_recv()

    @pl.when(jnp.logical_not(inside))
    def _():
        for h in range(n_core):
            for i in range(2):
                frames[i, h, halo_at, :] = jnp.zeros((HALO, half), BF)

    @pl.when(jnp.logical_not(first_half & has_prv))
    def _():
        docs[1] = docs[0]

    @pl.when(first_half | jnp.logical_not(has_nxt))
    def _():
        docs[2] = docs[0]

    for load in weights:
        load.start()

    own, before_docs, after_docs = docs[0], docs[1], docs[2]
    wide = (8, block)

    def row(x):
        return jnp.broadcast_to(x.astype(F32), wide)

    cur = row(jnp.where(first_half, own[0:1], own[1:2]))
    left = row(jnp.where(first_half, before_docs[1:2], own[0:1]))
    right = row(jnp.where(first_half, own[1:2], after_docs[0:1]))
    lanes = lax.broadcasted_iota(jnp.int32, wide, 1)
    before = jnp.where(lanes == 0, pltpu.roll(left, 1, 1), pltpu.roll(cur, 1, 1))
    after = jnp.where(lanes == block - 1, pltpu.roll(right, block - 1, 1), pltpu.roll(cur, block - 1, 1))
    position = (me * n_core + core) * block + lanes
    has_before = (cur == before) & (position > 0)
    has_after = (cur == after) & (position < n_seq * n_core * block - 1)
    both = jnp.where(lax.broadcasted_iota(jnp.int32, wide, 0) == 0,
                     jnp.where(has_before, 1.0, 0.0), jnp.where(has_after, 1.0, 0.0))
    marks = jnp.concatenate([both] * (block // 8), axis=0).T
    keep_before, keep_after = marks[:, 0:1], marks[:, 1:2]

    for h in range(n_core):
        prod[...] = frames[1, h].astype(F32) * frames[0, h].astype(F32)
        conv = (
            taps_f[h, 0:1, :] * (prod[HALO - 1:HALO - 1 + block, :] * keep_before)
            + taps_f[h, 1:2, :] * prod[HALO:HALO + block, :]
            + taps_f[h, 2:3, :] * (prod[HALO + 1:HALO + 1 + block, :] * keep_after)
        )
        mixed[:, h * half:(h + 1) * half] = (go_f[h].astype(F32) * conv).astype(BF)

    project.wait()
    square = jnp.zeros((block, 128), F32)
    for q in range(width // wide_col):
        cols = slice(q * wide_col, (q + 1) * wide_col)
        value = stream[:, cols].astype(F32) + dot(mixed[...], wp[:, cols])
        hidden[:, cols] = value
        value = value * value
        for i in range(wide_col // 128):
            square = square + value[:, i * 128:(i + 1) * 128]
    scale = lax.rsqrt(jnp.sum(square, axis=1, keepdims=True) / width + 1e-05)

    def chunk(q):
        return pl.ds(*cuts[q])

    def z_up(h, q):
        b = z - h
        piece = zbuf.at[b, :, chunk(q)]
        return remote(piece, piece, z_send.at[0], z_recv.at[b, q], at_z(z + 1))

    def z_down(h, q):
        b = z + h
        piece = zbuf.at[b, :, chunk(q)]
        return remote(piece, piece, z_send.at[0], z_recv.at[b, q], at_z(z - 1))

    def normed(cols):
        return (hidden[:, cols] * scale * gain[:, cols]).astype(BF)

    side = slice(main, width)
    pslab[p] = normed(side)
    s_copies = [
        remote(pslab.at[p], pslab.at[p], s_send.at[0], s_recv.at[0], in_plane(lax.rem(p + i, n_plane)))
        for i in range(1, n_plane)
    ]
    for copy in s_copies:
        copy.start()
    for q in range(nc):
        zbuf[z, :, chunk(q)] = normed(chunk(q))

    for q in range(nc):
        @pl.when(z < nz - 1)
        def _():
            z_up(0, q).start()

        @pl.when(z > 0)
        def _():
            z_down(0, q).start()

    def pump(h, q):
        @pl.when(z >= h)
        def _():
            piece = zbuf.at[z - h, :, chunk(q)]
            remote(piece, piece, z_send.at[0], z_recv.at[z - h, q], at_z(z)).wait_recv()

            @pl.when(z < nz - 1)
            def _():
                z_up(h, q).start()

        @pl.when(z + h < nz)
        def _():
            piece = zbuf.at[z + h, :, chunk(q)]
            remote(piece, piece, z_send.at[0], z_recv.at[z + h, q], at_z(z)).wait_recv()

            @pl.when(z > 0)
            def _():
                z_down(h, q).start()

    def seat_of(source):
        return pl.multiple_of((lax.rem(source, n_core) * n_plane + source // n_core) * cap, HALO)

    my_seat = seat_of(rank)

    def a_copy(k, j, q):
        b = ordered(k)
        return remote(
            outgoing.at[k, pl.ds((j - 1) * cap, cap), chunk(q)], arrived.at[b, pl.ds(my_seat, cap), chunk(q)],
            a_send.at[0], a_recv.at[b], plane_peer(j))

    def a_all(k):
        b = ordered(k)
        return remote(outgoing.at[k], arrived.at[b, pl.ds(cap, rows - cap), pl.ds(0, main)],
                      a_send.at[0], a_recv.at[b], plane_peer(1))

    def r_copy(k, j, q):
        b = ordered(k)
        seat = seat_of(lax.rem(rank + peers - j, peers))
        return remote(
            arrived.at[b, pl.ds(seat, cap), chunk(q)], returned.at[b, pl.ds(j * cap, cap), chunk(q)],
            r_send.at[0], r_recv.at[b, q], plane_peer(peers - j))

    def r_all(k, q):
        b = ordered(k)
        return remote(
            arrived.at[b, pl.ds(cap, rows - cap), chunk(q)], returned.at[b, pl.ds(cap, rows - cap), chunk(q)],
            r_send.at[0], r_recv.at[b, q], plane_peer(1))

    def dispatch(k):
        b = ordered(k)

        for q in range(nc):
            if k:
                pump(k, q)
            cols = chunk(q)
            picked = dot(select[k], zbuf[b, :, cols]).astype(BF)
            arrived[b, pl.ds(my_seat, cap), cols] = picked[:cap]
            outgoing[k, :, cols] = picked[cap:]
            for j in range(1, peers):
                a_copy(k, j, q).start()

    lot = n_plane * cap
    side_ref = pl.ds(main, slab)
    my_lot = pl.multiple_of(core * lot, HALO)
    other_lot = pl.multiple_of(other * lot, HALO)

    def v_copy(b, c):
        return remote(
            outgoing2.at[b * n_core + c], arrived.at[z, pl.ds(my_lot, lot), side_ref],
            v_send.at[0], v_recv.at[z], {"sp": b * n_plane + p, "tp": c})

    def v_wait(b, count):
        piece = arrived.at[b, pl.ds(0, count * lot), side_ref]
        remote(piece, piece, v_send.at[0], v_recv.at[b], partner).wait_recv()

    def rest(ref):
        return ref.at[pl.ds(0, ref.shape[0] - 1)]

    def all_of(ref, send, recv):
        return remote(ref, ref, send, recv, partner)

    s_all = all_of(rest(pslab), s_send.at[0], s_recv.at[0])
    v_all = all_of(rest(outgoing2), v_send.at[0], v_recv.at[0])
    w_all = all_of(rest(returned2), w_send.at[0], w_recv.at[0])
    f_all = all_of(rest(partial2), f_send.at[0], f_recv.at[0])

    def side_pick():
        s_all.wait_recv()
        for q in range(n_plane):
            plane_slots(q)
            picked = dot(select2[q], pslab[q]).astype(BF)
            for b in range(nz):
                for c in range(n_core):
                    at = (b * n_core + c) * cap
                    outgoing2[b * n_core + c, q * cap:(q + 1) * cap, :] = picked[at:at + cap]
        arrived[z, pl.ds(my_lot, lot), side] = outgoing2[z * n_core + core]
        v_copy(z, other).start()

    def side_send(h):
        @pl.when(z + h < nz)
        def _():
            for c in range(n_core):
                v_copy(z + h, jnp.int32(c)).start()

        @pl.when(z >= h)
        def _():
            for c in range(n_core):
                v_copy(z - h, jnp.int32(c)).start()

    def w_copy(b, c):
        piece = arrived.at[b, pl.ds(pl.multiple_of(c * lot, HALO), lot), side_ref]
        return remote(piece, returned2.at[z * n_core + core], w_send.at[0], w_recv.at[0],
                      {"sp": b * n_plane + p, "tp": c})

    def f_copy(q):
        return remote(partial2.at[q], summed2.at[p], f_send.at[0], f_recv.at[0], in_plane(q))

    def side_combine():
        w_all.wait_recv()
        for q in range(n_plane):
            results = jnp.concatenate(
                [returned2[b, q * cap:(q + 1) * cap, :] for b in range(nz * n_core)], axis=0)
            total = dot(spread2[q], results)

            @pl.when(p == q)
            def _():
                hidden[:, side] = hidden[:, side] + total

            @pl.when(p != q)
            def _():
                partial2[q] = total.astype(BF)
                f_copy(jnp.int32(q)).start()

    fcol = tile_of(ff, 256)

    def expert(k):
        b = ordered(k)
        if k == 0:
            for load in weights:
                load.wait()
        a_all(k).wait_recv()

        @pl.loop(0, ff // fcol)
        def _(i):
            cols = pl.ds(pl.multiple_of(i * fcol, fcol), fcol)
            early[0, :, cols] = dot(arrived[b, :, 0:main], wg[0:main, cols])
            early[1, :, cols] = dot(arrived[b, :, 0:main], wu[0:main, cols])

        v_wait(b, n_core if k else n_core - 1)

        @pl.loop(0, ff // fcol)
        def _(i):
            cols = pl.ds(pl.multiple_of(i * fcol, fcol), fcol)
            gate = jnp.minimum(early[0, :, cols] + dot(arrived[b, :, side], wg[side, cols]), 7.0)
            upper = jnp.clip(early[1, :, cols] + dot(arrived[b, :, side], wu[side, cols]), -7.0, 7.0)
            act[:, cols] = ((upper + 1.0) * gate * jax.nn.sigmoid(1.702 * gate)).astype(BF)

        arrived[b, :, side] = dot(act[...], wd[:, side]).astype(BF)
        if k == 0:
            returned2[z * n_core + core] = arrived[z, pl.ds(my_lot, lot), side]
            w_copy(z, other).start()
        else:
            for c in range(n_core):
                w_copy(b, c).start()

        for q in range(nc):
            cols = chunk(q)
            arrived[b, :, cols] = dot(act[...], wd[:, cols]).astype(BF)
            returned[b, 0:cap, cols] = arrived[b, pl.ds(my_seat, cap), cols]
            if k == nz - 1:
                give(k, q)

    def give(k, q):
        for j in range(1, peers):
            r_copy(k, j, q).start()

    def chained(b):
        return ((b < z) & (z < nz - 1)) | ((b > z) & (z > 0))

    def p_copy(k, q):
        b = ordered(k)
        down = b < z
        seat = jnp.where(down & (b == z - 1), nz, b)
        return remote(partial.at[k - 1, :, chunk(q)], chain.at[seat, :, chunk(q)],
                      p_send.at[0], p_recv.at[seat, q], at_z(jnp.where(down, z - 1, z + 1)))

    def p_wait(seat, q):
        piece = chain.at[seat, :, chunk(q)]
        remote(piece, piece, p_send.at[0], p_recv.at[seat, q], at_z(z)).wait_recv()

    def combine(k):
        b = ordered(k)

        for q in range(nc):
            cols = chunk(q)
            r_all(k, q).wait_recv()
            total = dot(spread[k], returned[b, :, cols])
            if k == 0:
                hidden[:, cols] = hidden[:, cols] + total
            else:
                @pl.when(chained(b))
                def _():
                    p_wait(b, q)
                    partial[k - 1, :, cols] = (total + chain[b, :, cols].astype(F32)).astype(BF)

                @pl.when(jnp.logical_not(chained(b)))
                def _():
                    partial[k - 1, :, cols] = total.astype(BF)

                p_copy(k, q).start()

    def give_all(k, low, high):
        for q in range(low, high):
            give(k, q)

    dispatch(0)
    for copy in list_waits:
        copy.wait_recv()
    for k in range(1, nz):
        line_slots(k)
        if k == nz - 1:
            give_all(0, 0, nc // 2)
        dispatch(k)
        if k == 1:
            side_pick()
        side_send(k)
        if k < nz - 1:
            expert(k - 1)
    give_all(0, nc // 2, nc)
    expert(nz - 2)
    expert(nz - 1)
    for k in range(nz - 2, 0, -1):
        give_all(k, 0, nc)
    combine(nz - 1)
    side_combine()
    for k in range(nz - 2, -1, -1):
        combine(k)
    f_all.wait_recv()
    for q in range(n_plane):
        @pl.when(p != q)
        def _():
            hidden[:, side] = hidden[:, side] + summed2[q].astype(F32)
    out_ref[:, side] = hidden[:, side].astype(BF)

    for q in range(nc):
        cols = chunk(q)

        @pl.when(z > 0)
        def _():
            p_wait(z, q)
            hidden[:, cols] = hidden[:, cols] + chain[z, :, cols].astype(F32)

        @pl.when(z < nz - 1)
        def _():
            p_wait(nz, q)
            hidden[:, cols] = hidden[:, cols] + chain[nz, :, cols].astype(F32)

        out_ref[:, cols] = hidden[:, cols].astype(BF)

    for i, there in enumerate((has_nxt, has_prv)):
        @pl.when(there)
        def _():
            remote(halo_part, halo_part, h_send.at[i], h_recv.at[0], partner).wait_send()

    @pl.when((first_half & has_nxt) | (jnp.logical_not(first_half) & has_prv))
    def _():
        docs_next.wait_send()

    for copy in swap_waits + list_waits + [s_all, v_all, w_all, f_all]:
        copy.wait_send()
    middle = (z > 0) & (z < nz - 1)

    @pl.when(middle)
    def _():
        remote(chain, chain, z_send.at[0], z_recv.at[0, 0], partner).wait_send()

    @pl.when(jnp.logical_not(middle))
    def _():
        remote(chain.at[0], chain.at[0], z_send.at[0], z_recv.at[0, 0], partner).wait_send()

    remote(outgoing, outgoing, a_send.at[0], a_recv.at[0], partner).wait_send()
    remote(outgoing, outgoing, r_send.at[0], r_recv.at[0, 0], partner).wait_send()
    remote(partial, partial, p_send.at[0], p_recv.at[0, 0], partner).wait_send()


def layer(n_seq, nz, n_plane, n_core, cap, *args):
    tok, half = args[0].shape
    block, width = args[6].shape
    ff = args[10].shape[1]
    peers = n_plane * n_core
    rows = peers * cap
    topk = args[8].shape[0]
    channels = half * n_core
    frame = block + 2 * HALO
    slab = SLAB if width > 2 * SLAB else 128
    main = width - slab
    parts = main // 128
    nc = min(CHUNKS, parts)
    edges = [-(-parts * i // nc) * 128 for i in range(nc + 1)]
    cuts = [(a, b - a) for a, b in zip(edges, edges[1:])]
    lot = n_plane * cap
    hbm = pl.BlockSpec(memory_space=pl.ANY)
    vmem = pl.BlockSpec(memory_space=pltpu.VMEM)
    dma = pltpu.SemaphoreType.DMA
    return pl.pallas_call(
        functools.partial(layer_kernel, n_seq, nz, n_plane, n_core, cap, cuts, slab),
        out_shape=jax.ShapeDtypeStruct((block, width), BF),
        in_specs=[hbm] * len(args),
        out_specs=vmem,
        scratch_shapes=[
            pltpu.VMEM((width, ff), BF),
            pltpu.VMEM((width, ff), BF),
            pltpu.VMEM((ff, width), BF),
            pltpu.VMEM((channels, width), BF),
            pltpu.VMEM((3, tok, half), BF),
            pltpu.VMEM((2, n_core, frame, half), BF),
            pltpu.VMEM((n_core, block, half), BF),
            pltpu.VMEM((n_core,) + args[3].shape, F32),
            pltpu.VMEM((3, n_core, block), jnp.int32),
            pltpu.VMEM((frame, half), F32),
            pltpu.VMEM((block, channels), BF),
            pltpu.VMEM((block, width), BF),
            pltpu.VMEM((1, width), F32),
            pltpu.VMEM((block, width), F32),
            pltpu.VMEM((nz, topk, block), jnp.int32),
            pltpu.VMEM((nz, topk, block), F32),
            pltpu.VMEM((nz, rows, block), BF),
            pltpu.VMEM((nz, block, rows), BF),
            pltpu.VMEM((nz, block, main), BF),
            pltpu.VMEM((nz, rows - cap, main), BF),
            pltpu.VMEM((nz, rows, width), BF),
            pltpu.VMEM((rows, ff), BF),
            pltpu.VMEM((nz, rows, main), BF),
            pltpu.VMEM((nz - 1, block, main), BF),
            pltpu.VMEM((nz + 1, block, main), BF),
            pltpu.VMEM((2, rows, ff), F32),
            pltpu.VMEM((n_plane, topk, block), jnp.int32),
            pltpu.VMEM((n_plane, topk, block), F32),
            pltpu.VMEM((n_plane, nz * n_core * cap, block), BF),
            pltpu.VMEM((n_plane, block, nz * n_core * cap), BF),
            pltpu.VMEM((n_plane, block, slab), BF),
            pltpu.VMEM((nz * n_core, lot, slab), BF),
            pltpu.VMEM((nz * n_core, lot, slab), BF),
            pltpu.VMEM((n_plane, block, slab), BF),
            pltpu.VMEM((n_plane, block, slab), BF),
            dma((12,)), dma((3,)), dma((3,)), dma((2,)), dma((1,)),
            dma((1,)), dma((1,)), dma((2,)), dma((2,)),
            dma((1,)), dma((nz, nc)), dma((1,)), dma((nz,)), dma((1,)), dma((nz, nc)),
            dma((1,)), dma((nz + 1, nc)),
            dma((1,)), dma((1,)), dma((1,)), dma((nz,)), dma((1,)), dma((1,)), dma((1,)), dma((1,)),
        ],
        compiler_params=pltpu.CompilerParams(
            collective_id=0, has_side_effects=True, vmem_limit_bytes=62 * 2**20),
        name="mixer_experts",
    )(*args)


def per_device(
    conv_in, gate_outer, gate_inner, tap_weights, doc_ids, w_proj, stream, norm_gain,
    routes, route_weights, w_gate, w_up, w_down,
):
    n_seq = lax.axis_size("sp")
    n_core = lax.axis_size("tp")
    tok_dev = conv_in.shape[0]
    topk = routes.shape[1]
    capacity = max(2, 2 * tok_dev * topk // (n_core * n_seq * n_core))
    capacity = -(-capacity // 16) * 16
    nz = max(d for d in range(1, math.isqrt(n_seq) + 1) if n_seq % d == 0)
    return layer(
        n_seq, nz, n_seq // nz, n_core, capacity,
        conv_in, gate_outer, gate_inner, tap_weights,
        doc_ids.reshape(n_core, tok_dev // n_core), w_proj, stream, norm_gain.reshape(1, -1),
        routes.T, route_weights.T, w_gate[0], w_up[0], w_down[0])


def solution(mesh):
    in_specs = (
        P("sp", "tp"),
        P("sp", "tp"),
        P("sp", "tp"),
        P(None, "tp"),
        P("sp"),
        P(),
        P(("sp", "tp"), None),
        P(),
        P(("sp", "tp"), None),
        P(("sp", "tp"), None),
        P(("sp", "tp"), None, None),
        P(("sp", "tp"), None, None),
        P(("sp", "tp"), None, None),
    )
    return jax.shard_map(
        per_device, mesh=mesh, in_specs=in_specs, out_specs=P(("sp", "tp"), None), check_vma=False
    )
```
